32 devices in a mesh: sp: 16 (over z, y, core), tp: 2 (over x).
Axes of the slice: x: 2, y: 2, z: 4, core: 2. Of those that a mesh axis runs over, the one named last changes fastest.
Arguments:
- tokens: bfloat16 [8192, 2048], P(('sp', 'tp')), may hold values from -6 to 6
- norm_gain: float32 [2048], replicated, may hold values from 0.1 to 1.9
- query_weight: bfloat16 [2048, 1024], P(None, 'tp'), may hold values from -0.13258252 to 0.13258252
- key_weight: bfloat16 [2048, 1024], P(None, 'tp'), may hold values from -0.13258252 to 0.13258252
- value_weight: bfloat16 [2048, 1024], P(None, 'tp'), may hold values from -0.125 to 0.125
- glu_value_weight: bfloat16 [2048, 1024], P(None, 'tp'), may hold values from -0.125 to 0.125
- glu_gate_weight: bfloat16 [2048, 1024], P(None, 'tp'), may hold values from -0.125 to 0.125
- qk_gain: float32 [2, 64], replicated, may hold values from 1 to 6
- mix_lambda: float32 [8], P('tp'), may hold values from 0.3 to 0.8
- head_gain: float32 [128], replicated, may hold values from 0.1 to 1.9
- conv_kernel: float32 [31, 1024], P(None, 'tp'), may hold values from -1 to 1
- channel_gain: float32 [1024], P('tp'), may hold values from 0.1 to 1.9
- channel_shift: float32 [1024], P('tp'), may hold values from -3 to 3
- output_weight: bfloat16 [2048, 2048], replicated, may hold values from -0.125 to 0.125
Outputs:
- mixed: bfloat16 [8192, 2048], P(('sp', 'tp'))
- log_totals: float32 [2, 8, 8192], P(None, 'tp', 'sp')
The draws below stay inside these ranges and needn't reach their ends.
All inputs are finite; a program needn't handle non-finite values.
Results may differ from the reference program's by a relative error of at most 0.035.
Values may be sent and summed in bfloat16 or wider, within the bound.
A program may use at most 128 MiB of HBM per device.

```python
import jax
import jax.numpy as jnp
from jax import lax

D = 2048
HEADS = 8
HEAD_DIM = 64
VDIM = 128
CONV = 1024
KERNEL = 31
TOKENS = 8192
MIX = 2048


def draw_qk_gain(key, part):
    spread = jax.random.uniform(jax.random.fold_in(key, 7), (2, HEAD_DIM), jnp.float32, -1.0, 1.0)
    return 1.3 + 0.25 * spread


def paired_weights(key):
    columns = HEADS * 2 * HEAD_DIM
    factor = D ** (-0.5)
    limit = 6.0 * factor
    shared = jax.random.normal(jax.random.fold_in(key, 11), (D, columns), jnp.float32) * factor
    separate = jax.random.normal(jax.random.fold_in(key, 12), (D, columns), jnp.float32) * factor
    shared = jnp.clip(shared, -limit, limit)
    separate = jnp.clip(separate, -limit, limit)
    return (shared, separate)


def draw_query_weight(key, part):
    shared, separate = paired_weights(key)
    return shared.astype(jnp.bfloat16)


def draw_key_weight(key, part):
    shared, separate = paired_weights(key)
    return separate.astype(jnp.bfloat16)


def block_levels(rng, dims, pieces, low, largest):
    def one(position, blocks):
        draws = jax.random.uniform(jax.random.fold_in(jax.random.fold_in(rng, 6), position), (blocks,), jnp.float32, low / len(pieces), largest / len(pieces))
        return jnp.repeat(jnp.exp(draws), dims[position] // blocks).reshape((-1,) + (1,) * (len(dims) - position - 1))

    factor_of = one(*pieces[0])
    for cut in pieces[1:]:
        factor_of = factor_of * one(*cut)
    return factor_of


def normal_values(own_key, shape, width, most, split=(), held_as=jnp.bfloat16):
    drawn = width * jax.random.normal(own_key, shape, jnp.float32)
    if split:
        drawn = drawn * block_levels(own_key, shape, split, -0.22, 0.18)
    return jnp.clip(drawn, -most, most).astype(held_as)


def setup_inputs(seed: int = 0) -> dict:
    splits = jax.random.split(jax.random.key(seed), 15)
    tokens = normal_values(splits[0], (TOKENS, D), 1.0, 6.0, ((0, 32),))
    norm_gain = jnp.clip(1.0 + 0.18 * jax.random.normal(splits[1], (D,), jnp.float32), 0.1, 1.9)
    query_weight = draw_query_weight(jax.random.fold_in(splits[14], 71), 0)
    key_weight = draw_key_weight(jax.random.fold_in(splits[14], 71), 0)
    value_weight = normal_values(splits[4], (D, HEADS * VDIM), D ** -0.5, 0.125, ((1, 2),))
    glu_value_weight = normal_values(splits[5], (D, CONV), D ** -0.5, 0.125, ((1, 2),))
    glu_gate_weight = normal_values(splits[6], (D, CONV), D ** -0.5, 0.125, ((1, 2),))
    qk_gain = draw_qk_gain(jax.random.fold_in(splits[14], 71), 0)
    mix_lambda = jnp.clip(0.3 + 0.5 * jax.random.uniform(splits[8], (HEADS,), jnp.float32) ** block_levels(splits[8], (HEADS,), ((0, 2),), -0.2, 0.2), 0.3, 0.8)
    head_gain = jnp.clip(1.0 + 0.18 * jax.random.normal(splits[9], (VDIM,), jnp.float32), 0.1, 1.9)
    conv_kernel = normal_values(splits[10], (KERNEL, CONV), KERNEL ** -0.5, 1.0, ((1, 2),), jnp.float32)
    channel_gain = jnp.clip(1.0 + 0.18 * jax.random.normal(splits[11], (CONV,), jnp.float32), 0.1, 1.9)
    channel_shift = normal_values(splits[12], (CONV,), 0.5, 3.0, ((0, 2),), jnp.float32)
    output_weight = normal_values(splits[13], (MIX, D), MIX ** -0.5, 0.125)
    return dict(tokens=tokens, norm_gain=norm_gain, query_weight=query_weight, key_weight=key_weight, value_weight=value_weight, glu_value_weight=glu_value_weight, glu_gate_weight=glu_gate_weight, qk_gain=qk_gain, mix_lambda=mix_lambda, head_gain=head_gain, conv_kernel=conv_kernel, channel_gain=channel_gain, channel_shift=channel_shift, output_weight=output_weight)


def rotate(values, positions):
    half = values.shape[-1] // 2
    inverse = 10000.0 ** (-jnp.arange(0, half, dtype=jnp.float32) * 2.0 / values.shape[-1])
    angles = positions[:, None] * inverse[None, :]
    cosine = jnp.cos(angles)[:, None, None, :]
    sine = jnp.sin(angles)[:, None, None, :]
    first = values[..., :half]
    second = values[..., half:]
    return jnp.concatenate([first * cosine - second * sine, second * cosine + first * sine], axis=-1)

def prepare(raw, qk_gain, positions):
    values = raw.astype(jnp.float32)
    values = values * lax.rsqrt(lax.optimization_barrier(jnp.mean(values * values, axis=-1, keepdims=True)) + 1e-06)
    values = values * qk_gain[None, None, :, :]
    return rotate(values, positions).astype(jnp.bfloat16)

def reference(tokens, norm_gain, query_weight, key_weight, value_weight, glu_value_weight, glu_gate_weight, qk_gain, mix_lambda, head_gain, conv_kernel, channel_gain, channel_shift, output_weight):
    inputs = tokens.astype(jnp.float32)
    normed = (inputs * lax.rsqrt(lax.optimization_barrier(jnp.mean(inputs * inputs, axis=-1, keepdims=True)) + 1e-06) * norm_gain).astype(jnp.bfloat16)
    queries = jnp.dot(normed, query_weight, preferred_element_type=jnp.float32).astype(jnp.bfloat16).reshape(TOKENS, HEADS, 2, HEAD_DIM)
    keys = jnp.dot(normed, key_weight, preferred_element_type=jnp.float32).astype(jnp.bfloat16).reshape(TOKENS, HEADS, 2, HEAD_DIM)
    values = jnp.dot(normed, value_weight, preferred_element_type=jnp.float32).astype(jnp.bfloat16).reshape(TOKENS, HEADS, VDIM)
    glu_a = jnp.dot(normed, glu_value_weight, preferred_element_type=jnp.float32).astype(jnp.bfloat16)
    glu_g = jnp.dot(normed, glu_gate_weight, preferred_element_type=jnp.float32).astype(jnp.bfloat16)
    positions = jnp.arange(TOKENS, dtype=jnp.int32)
    rq = prepare(queries, qk_gain, positions.astype(jnp.float32))
    rk = prepare(keys, qk_gain, positions.astype(jnp.float32))
    key_heads = jnp.transpose(rk, (1, 0, 2, 3)).astype(jnp.float32)
    value_heads = jnp.transpose(values, (1, 0, 2)).astype(jnp.float32)
    block = 512
    blocks = TOKENS // block
    query_blocks = rq.reshape(blocks, block, HEADS, 2, HEAD_DIM)
    starts = jnp.arange(blocks, dtype=jnp.int32) * block
    scale = HEAD_DIM ** (-0.5)

    def one_block(item):
        query_block, begin = item
        query_pos = begin + jnp.arange(block, dtype=jnp.int32)
        allowed = positions[None, :] <= query_pos[:, None]

        def one_head(head_item):
            query_head, key_head, value_head, weight_two = head_item
            scores = jnp.einsum('qmd,kmd->mqk', query_head.astype(jnp.float32), key_head) * scale
            scores = jnp.where(allowed[None], scores, -1e+30)
            top = lax.optimization_barrier(jnp.max(scores, axis=-1))
            probs = jnp.where(allowed[None], jnp.exp(scores - top[..., None]), 0.0)
            total = lax.optimization_barrier(jnp.sum(probs, axis=-1))
            rounded = probs.astype(jnp.bfloat16).astype(jnp.float32)
            summed = jnp.einsum('mqk,kd->mqd', rounded, value_head)
            heads_out = summed[0] / total[0][:, None] - weight_two * summed[1] / total[1][:, None]
            heads_out = heads_out * lax.rsqrt(lax.optimization_barrier(jnp.mean(heads_out * heads_out, axis=-1, keepdims=True)) + 1e-06) * head_gain
            return (heads_out.astype(jnp.bfloat16), top + jnp.log(total))
        return lax.map(one_head, (jnp.transpose(query_block, (1, 0, 2, 3)), key_heads, value_heads, mix_lambda))
    outputs, totals = lax.map(one_block, (query_blocks, starts))
    attended = jnp.transpose(outputs, (0, 2, 1, 3)).reshape(TOKENS, HEADS * VDIM)
    log_totals = jnp.transpose(totals, (2, 1, 0, 3)).reshape(2, HEADS, TOKENS)
    gated = (glu_a.astype(jnp.float32) * jax.nn.sigmoid(glu_g.astype(jnp.float32))).astype(jnp.bfloat16)
    padded = jnp.concatenate([jnp.zeros((KERNEL - 1, CONV), jnp.float32), gated.astype(jnp.float32)], axis=0)
    convolved = jnp.zeros((TOKENS, CONV), jnp.float32)
    for offset in range(KERNEL):
        convolved = convolved + conv_kernel[offset][None, :] * padded[offset:offset + TOKENS]
    middle = lax.optimization_barrier(jnp.mean(convolved, axis=-1, keepdims=True))
    spread = lax.optimization_barrier(jnp.mean(convolved * convolved, axis=-1, keepdims=True)) - middle * middle
    conv_out = jax.nn.silu((convolved - middle) * lax.rsqrt(spread + 1e-05) * channel_gain + channel_shift).astype(jnp.bfloat16)
    merged = jnp.concatenate([attended, conv_out], axis=1)
    mixed = jnp.dot(merged, output_weight, preferred_element_type=jnp.float32).astype(jnp.bfloat16)
    return (mixed, log_totals)
```

```python
import math

import jax
import jax.numpy as jnp
from jax import lax
from jax.experimental import pallas as pl
from jax.experimental.pallas import tpu as pltpu
from jax.sharding import PartitionSpec as P

MESH = pl.DeviceIdType.MESH
NEG = -1e30


def from_behind(value, axis, steps):
    count = lax.axis_size(axis)
    leading, last = (max(0, -steps), min(count, count - steps))
    return lax.ppermute(value, axis, [(source, source + steps) for source in range(leading, last)])


def flipped(g, a, group):
    if group % 2:
        return g
    return jnp.where(a % 2 == 0, g, group - 1 - g)


def spread_kernel(ways, group, q_ref, kv_ref, qo_ref, kvo_ref, qsend, qrecv, ksend, kfwd, krelay, krecv, local):
    me = lax.axis_index("sp")
    a = me // group
    g = me % group
    cores = 2 if group % 2 == 0 else 1
    half = group // cores
    mate = a * group + (g + 1 - 2 * (g % 2)) if cores == 2 else me

    def same(d):
        return (g + d * cores) % group

    peers = [lax.rem(a + d, ways) * group + g for d in range(1, ways)]
    peers += [a * group + same(d) for d in range(1, half)]
    if cores == 2:
        peers.append(mate)
        peers += [lax.rem(a + d, ways) * group + group - 1 - g for d in range(ways)]
    barrier = pltpu.get_barrier_semaphore()
    for peer in peers:
        pl.semaphore_signal(barrier, inc=1, device_id={"sp": peer}, device_id_type=MESH)
    pl.semaphore_wait(barrier, len(peers))

    def kv_copy(src, slot, send, peer):
        return pltpu.make_async_remote_copy(
            src_ref=src, dst_ref=kvo_ref.at[slot], send_sem=send, recv_sem=krecv.at[slot],
            device_id={"sp": peer}, device_id_type=MESH)

    sends = []
    keep = pltpu.make_async_copy(kv_ref.at[a], kvo_ref.at[me], local.at[0])
    keep_q = pltpu.make_async_copy(q_ref.at[a], qo_ref.at[a], local.at[1])
    keep.start()

    def q_copy(h, slot, d):
        return pltpu.make_async_remote_copy(
            src_ref=q_ref.at[h], dst_ref=qo_ref.at[slot], send_sem=qsend.at[d], recv_sem=qrecv.at[slot],
            device_id={"sp": h * group + flipped(g, a, group)}, device_id_type=MESH)

    stays = a % 2 == 0 if cores == 2 else a >= 0

    @pl.when(stays)
    def _():
        keep_q.start()
    order = list(range(1, ways))
    for d in order:
        h = lax.rem(a + d, ways)
        c = kv_copy(kv_ref.at[h], me, ksend.at[d - 1], h * group + g)
        c.start()
        sends.append(c)

    def forward(d):
        src_a = lax.rem(a + ways - d, ways)
        slot = src_a * group + g
        if d:
            kv_copy(kvo_ref.at[slot], slot, ksend.at[d - 1], me).wait_recv()
            src = kvo_ref.at[slot]
        else:
            src = kv_ref.at[a]
        n = 0
        for e in range(1, half):
            c = kv_copy(src, slot, kfwd.at[d, n], a * group + same(e))
            c.start()
            sends.append(c)
            n += 1
        if cores == 2:
            c = kv_copy(src, slot, kfwd.at[d, n], mate)
            c.start()
            sends.append(c)

    def relay(d):
        src_a = lax.rem(a + ways - d, ways)
        for e in range(1, half):
            slot = src_a * group + same(e)
            kv_copy(kvo_ref.at[slot], slot, krelay.at[d, e - 1], mate).wait_recv()
            if cores == 2:
                c = kv_copy(kvo_ref.at[slot], slot, krelay.at[d, e - 1], mate)
                c.start()
                sends.append(c)

    forward(0)
    for d in order:
        c = q_copy(lax.rem(a + d, ways), a, d)
        c.start()
        sends.append(c)
    if cores == 2:
        @pl.when(jnp.logical_not(stays))
        def _():
            q_copy(a, a, 0).start()
    for d in range(1, ways):
        forward(d)
        relay(d - 1)
    relay(ways - 1)
    if cores == 2:
        for d in range(ways):
            src_a = lax.rem(a + ways - d, ways)
            for e in range(half):
                slot = src_a * group + (g + 1 - 2 * (g % 2) + e * cores) % group
                kv_copy(kvo_ref.at[slot], slot, krelay.at[0, 0], mate).wait_recv()
    for d in range(1, ways):
        src_a = lax.rem(a + ways - d, ways)
        q_copy(a, src_a, d).wait_recv()
    for c in sends:
        c.wait_send()
    keep.wait()

    @pl.when(stays)
    def _():
        keep_q.wait()

    if cores == 2:
        @pl.when(jnp.logical_not(stays))
        def _():
            q_copy(a, a, 0).wait()


def spread(q, kv, ways, group):
    cores = 2 if group % 2 == 0 else 1
    half = group // cores
    any_ = pl.BlockSpec(memory_space=pl.ANY)
    n = max(ways - 1, 1)
    return pl.pallas_call(
        lambda *refs: spread_kernel(ways, group, *refs),
        out_shape=(
            jax.ShapeDtypeStruct(q.shape, q.dtype),
            jax.ShapeDtypeStruct((ways * group,) + kv.shape[1:], kv.dtype),
        ),
        in_specs=[any_, any_],
        out_specs=(any_, any_),
        scratch_shapes=[
            pltpu.SemaphoreType.DMA((ways,)),
            pltpu.SemaphoreType.DMA((ways,)),
            pltpu.SemaphoreType.DMA((n,)),
            pltpu.SemaphoreType.DMA((ways, half)),
            pltpu.SemaphoreType.DMA((ways, max(half - 1, 1))),
            pltpu.SemaphoreType.DMA((ways * group,)),
            pltpu.SemaphoreType.DMA((2,)),
        ],
        compiler_params=pltpu.CompilerParams(collective_id=1, has_side_effects=True),
        name="spread",
    )(q, kv)


def collect_kernel(ways, group, tp, att_ref, lt_ref, conv_ref, ao_ref, lo_ref, co_ref, asend, arecv, lsend, lrecv, csend, crecv, local):
    me = lax.axis_index("sp")
    t = lax.axis_index("tp")
    a = me // group
    g = me % group
    vdim = att_ref.shape[-1]
    cch = conv_ref.shape[-1]

    def coords(i):
        dt, da = i % tp, i // tp
        return lax.rem(a + da, ways), lax.rem(t + dt, tp)

    total = ways * tp
    both = group % 2 == 0
    barrier = pltpu.get_barrier_semaphore()
    for i in range(total):
        pa, pt = coords(i)
        if i:
            pl.semaphore_signal(barrier, inc=1, device_id={"sp": pa * group + g, "tp": pt}, device_id_type=MESH)
        if both:
            pl.semaphore_signal(
                barrier, inc=1, device_id={"sp": pa * group + group - 1 - g, "tp": pt}, device_id_type=MESH)
    pl.semaphore_wait(barrier, 2 * total - 1 if both else total - 1)

    head = t * ways + a

    def att_copy(i, slot):
        pa, pt = coords(i)
        return pltpu.make_async_remote_copy(
            src_ref=att_ref.at[pa, pt], dst_ref=ao_ref.at[slot], send_sem=asend.at[i], recv_sem=arecv.at[slot],
            device_id={"sp": pa * group + flipped(g, pa, group), "tp": pt}, device_id_type=MESH)

    def lt_copy(i, slot):
        pa = lax.rem(a + i, ways)
        return pltpu.make_async_remote_copy(
            src_ref=lt_ref.at[pa], dst_ref=lo_ref.at[slot], send_sem=lsend.at[i], recv_sem=lrecv.at[slot],
            device_id={"sp": pa * group + flipped(g, pa, group), "tp": t}, device_id_type=MESH)

    stays = a % 2 == 0 if both else a >= 0
    sends = []
    for i in range(total - 1, 0, -1):
        c = att_copy(i, head)
        c.start()
        sends.append(c)
    for i in range(1, tp):
        pa, pt = coords(i)
        c = pltpu.make_async_remote_copy(
            src_ref=conv_ref.at[pt], dst_ref=co_ref.at[t],
            send_sem=csend.at[i], recv_sem=crecv.at[t],
            device_id={"sp": me, "tp": pt}, device_id_type=MESH)
        c.start()
        sends.append(c)
    for i in range(1, ways):
        c = lt_copy(i, a)
        c.start()
        sends.append(c)
    keep = pltpu.make_async_copy(conv_ref.at[t], co_ref.at[t], local.at[1])
    keep.start()
    mine = [
        pltpu.make_async_copy(att_ref.at[a, t], ao_ref.at[head], local.at[0]),
        pltpu.make_async_copy(lt_ref.at[a], lo_ref.at[a], local.at[2]),
    ]

    @pl.when(stays)
    def _():
        for c in mine:
            c.start()

    if both:
        @pl.when(jnp.logical_not(stays))
        def _():
            att_copy(0, head).start()
            lt_copy(0, a).start()
    for i in range(1, total):
        pa, pt = coords(i)
        att_copy(i, pt * ways + pa).wait_recv()
    for i in range(1, tp):
        pa, pt = coords(i)
        pltpu.make_async_remote_copy(
            src_ref=conv_ref.at[t], dst_ref=co_ref.at[pt],
            send_sem=csend.at[i], recv_sem=crecv.at[pt],
            device_id={"sp": me, "tp": pt}, device_id_type=MESH).wait_recv()
    for i in range(1, ways):
        lt_copy(i, lax.rem(a + i, ways)).wait_recv()
    for c in sends:
        c.wait_send()
    keep.wait()

    @pl.when(stays)
    def _():
        for c in mine:
            c.wait()

    if both:
        @pl.when(jnp.logical_not(stays))
        def _():
            att_copy(0, head).wait()
            lt_copy(0, a).wait()


def collect(att, lt, conv, ways, group, tp):
    any_ = pl.BlockSpec(memory_space=pl.ANY)
    rows, vdim = att.shape[2:]
    total = ways * tp
    return pl.pallas_call(
        lambda *refs: collect_kernel(ways, group, tp, *refs),
        out_shape=(
            jax.ShapeDtypeStruct((total, rows, vdim), att.dtype),
            jax.ShapeDtypeStruct(lt.shape, lt.dtype),
            jax.ShapeDtypeStruct(conv.shape, conv.dtype),
        ),
        in_specs=[any_] * 3,
        out_specs=(any_,) * 3,
        scratch_shapes=[
            pltpu.SemaphoreType.DMA((total,)),
            pltpu.SemaphoreType.DMA((total,)),
            pltpu.SemaphoreType.DMA((ways,)),
            pltpu.SemaphoreType.DMA((ways,)),
            pltpu.SemaphoreType.DMA((tp,)),
            pltpu.SemaphoreType.DMA((tp,)),
            pltpu.SemaphoreType.DMA((3,)),
        ],
        compiler_params=pltpu.CompilerParams(collective_id=2, has_side_effects=True),
        name="collect",
    )(att, lt, conv)


def attention(place, lam, head_gain, qt, kv, tile=512):
    ways, qdim, rows = qt.shape
    hd = qdim // 2
    blocks = kv.shape[0]
    vdim = head_gain.shape[0]
    group = blocks // ways
    tile = math.gcd(tile, rows)
    tiles = rows // tile
    def kernel(place_ref, lam_ref, gain_ref, q_ref, kv_ref, o_ref, lt_ref, sa, sb, acc_ref):
        i = pl.program_id(0); s = pl.program_id(1)
        chunk = i * group + flipped(place_ref[0], i, group)
        qs = [q_ref[0, m * hd:(m + 1) * hd, :] for m in range(2)]
        def score(j, ref):
            for m in range(2):
                ref[m] = jnp.dot(kv_ref[j, :rows, m * hd:(m + 1) * hd], qs[m], preferred_element_type=jnp.float32)
        def absorb(j, ref, tops, masked=False):
            vb = jnp.concatenate([kv_ref[j, rows + b * vdim:rows + (b + 1) * vdim] for b in range(rows // 128)], axis=1)
            vb = jnp.concatenate([vb, jnp.ones((16, rows), jnp.bfloat16)], axis=0)
            out=[]
            for m in range(2):
                sc = ref[m]
                if masked:
                    kp = lax.broadcasted_iota(jnp.int32, sc.shape, 0)
                    qp = lax.broadcasted_iota(jnp.int32, sc.shape, 1) + s * tile
                    sc = jnp.where(kp <= qp, sc, NEG)
                new = jnp.maximum(tops[m], jnp.max(sc, axis=0, keepdims=True))
                p = jnp.exp(sc - new)
                f = jnp.exp(tops[m] - new)
                acc_ref[m] = acc_ref[m] * f + jnp.dot(vb, p.astype(jnp.bfloat16), preferred_element_type=jnp.float32)
                out.append(new)
            return tuple(out)
        acc_ref[...] = jnp.zeros_like(acc_ref)
        one = jnp.full((1, tile), NEG, jnp.float32)
        score(chunk, sa)
        score(0, sb)
        tops = absorb(chunk, sa, (one, one), True)

        def pair(j, tops):
            score(2 * j + 1, sa)
            tops = absorb(2 * j, sb, tops)
            score(2 * j + 2, sb)
            return absorb(2 * j + 1, sa, tops)

        tops = lax.fori_loop(0, chunk // 2, pair, tops)
        tops = lax.cond(chunk % 2 == 1, lambda t: absorb(chunk - 1, sb, t), lambda t: t, tops)
        a0=acc_ref[0]; a1=acc_ref[1]
        t0,t1=tops
        l0=a0[vdim:vdim+1]; l1=a1[vdim:vdim+1]; a0=a0[:vdim]; a1=a1[:vdim]
        heads = a0 / l0 - lam_ref[0] * a1 / l1
        heads = heads * lax.rsqrt(jnp.mean(heads * heads, axis=0, keepdims=True) + 1e-06) * gain_ref[...]
        o_ref[0] = heads.T.astype(jnp.bfloat16)
        lt_ref[0, 0:1, :] = t0 + jnp.log(l0)
        lt_ref[0, 1:2, :] = t1 + jnp.log(l1)
    smem = pl.BlockSpec(memory_space=pltpu.SMEM)
    return pl.pallas_call(kernel, grid=(ways, tiles),
        out_shape=(jax.ShapeDtypeStruct((ways, rows, vdim), jnp.bfloat16), jax.ShapeDtypeStruct((ways, 2, rows), jnp.float32)),
        in_specs=[smem, smem, pl.BlockSpec((vdim, 1), lambda i, s: (0, 0)), pl.BlockSpec((1, qdim, tile), lambda i, s: (i, 0, s)), pl.BlockSpec(kv.shape, lambda i, s: (0, 0, 0))],
        out_specs=(pl.BlockSpec((1, tile, vdim), lambda i, s: (i, s, 0)), pl.BlockSpec((1, 2, tile), lambda i, s: (i, 0, s))),
        scratch_shapes=[pltpu.VMEM((2,rows,tile),jnp.float32),pltpu.VMEM((2,rows,tile),jnp.float32),pltpu.VMEM((2,vdim+16,tile),jnp.float32)],
        compiler_params=pltpu.CompilerParams(vmem_limit_bytes=58 << 20), name="attend")(place, lam, head_gain.reshape(-1, 1), qt, kv)


def prepare_t(raw, qk_gain, cosine, sine):
    values = raw.astype(jnp.float32)
    values = values * lax.rsqrt(jnp.mean(values * values, axis=2, keepdims=True) + 1e-06)
    values = values * qk_gain[None, :, :, None]
    half = raw.shape[2] // 2
    first, second = values[:, :, :half], values[:, :, half:]
    return jnp.concatenate(
        [first * cosine - second * sine, second * cosine + first * sine], axis=2
    ).astype(jnp.bfloat16)

PIECES = 4


def layer_kernel(
    sizes, tokens_ref, gain_ref, wq_ref, wk_ref, wv_ref, wa_ref, wg_ref, tab_ref, lam_ref, hgain_ref, taps_ref,
    cgain_ref, cshift_ref, wo_ref, mixed_ref, lo_ref,
    toks, w, tab, wo, nrm, raw, qs, kvs, qbuf, kvbuf, gext, glast, halo, conv, cvo, cvr, st, str_, macc,
    sa, sb, acc, aos, ao, lts, lor,
    load, tok_send, tok_recv, q_send, q_recv, kv_send, kv_recv, y_send, m_send, halo_send, halo_recv,
    st_send, st_recv, cv_send, cv_recv, ao_send, ao_recv, lt_send, lt_recv,
):
    ways, group, tp, taps = sizes
    s = lax.axis_index("sp")
    t = lax.axis_index("tp")
    a = s // group
    g = s % group
    sp = ways * group
    other = 1 - t
    prow = nrm.shape[0]
    rows = PIECES * prow
    hd = qbuf.shape[2] // 2
    vdim = hgain_ref.shape[1]
    cch = conv.shape[2]
    channels = cch * tp
    half = hd // 2
    mate = a * group + g + 1 - 2 * (g % 2)
    across = a * group + (g + 2) % group
    stays = a % 2 == 0

    def turn(i):
        return g + (i % 2) * (group - 1 - 2 * g)

    def remote(src, dst, send, recv, row, col):
        return pltpu.make_async_remote_copy(
            src_ref=src, dst_ref=dst, send_sem=send, recv_sem=recv,
            device_id={"sp": row, "tp": col}, device_id_type=MESH)

    loads = [pltpu.make_async_copy(tokens_ref.at[pl.ds(j * prow, prow)], toks.at[j], load.at[j]) for j in range(2)]
    loads += [
        pltpu.make_async_copy(ref, w.at[n], load.at[2 + n]) for n, ref in enumerate((wq_ref, wk_ref, wv_ref, wa_ref, wg_ref))]
    loads.append(pltpu.make_async_copy(tab_ref, tab, load.at[7]))
    out_load = pltpu.make_async_copy(wo_ref, wo, load.at[8])
    for c in loads:
        c.start()
    out_load.start()

    barrier = pltpu.get_barrier_semaphore()
    flat = s * tp + t

    def greet(n, carry):
        to = lax.rem(flat + n, sp * tp)
        pl.semaphore_signal(barrier, inc=1, device_id={"sp": to // tp, "tp": to % tp}, device_id_type=MESH)
        return carry

    lax.fori_loop(1, sp * tp, greet, 0)
    pl.semaphore_wait(barrier, sp * tp - 1)

    def tok_copy(j):
        return remote(
            tokens_ref.at[pl.ds(j * prow, prow)], toks.at[2 + j], tok_send.at[j], tok_recv.at[j], s, other)

    for j in range(2):
        tok_copy(j).start()

    def piece_of(n):
        return (t + (n // 2) * (1 - 2 * t)) * 2 + n % 2

    def kv_z(pc, d):
        h = lax.rem(a + d, ways)
        return remote(kvs.at[pc, h], kvbuf.at[s, pc], kv_send.at[pc, d - 1], kv_recv.at[s, pc], h * group + g, t)

    def q_z(pc, d):
        h = lax.rem(a + d, ways)
        return remote(qs.at[pc, h], qbuf.at[a, pc], q_send.at[pc, d], q_recv.at[a, pc], h * group + turn(a), t)

    def kv_wait(slot, pc):
        remote(kvs.at[pc, 0], kvbuf.at[slot, pc], kv_send.at[0, 0], kv_recv.at[slot, pc], s, other).wait_recv()

    def to_across(src, slot, pc, d):
        return remote(src, kvbuf.at[slot, pc], y_send.at[d, pc], kv_recv.at[slot, pc], across, t)

    def to_mate(src, slot, pc, d):
        return remote(src, kvbuf.at[slot, pc], m_send.at[d, pc], kv_recv.at[slot, pc], mate, t)

    def prepared(x, scale, pc):
        outs = []
        for m in range(2):
            f = x[m * hd:m * hd + half]
            b = x[m * hd + half:(m + 1) * hd]
            mean = (jnp.sum(f * f, axis=0, keepdims=True) + jnp.sum(b * b, axis=0, keepdims=True)) / hd
            r = lax.rsqrt(mean + 1e-06) * scale
            f = f * r
            b = b * r
            outs.append(f * tab[pc, m, 0] - b * tab[pc, m, 1])
            outs.append(b * tab[pc, m, 2] + f * tab[pc, m, 3])
        return jnp.concatenate(outs, axis=0)

    def relay_z(n):
        pc = piece_of(n)
        for d in range(1, ways):
            slot = lax.rem(a + ways - d, ways) * group + g
            kv_wait(slot, pc)
            to_across(kvbuf.at[slot, pc], slot, pc, d).start()
            to_mate(kvbuf.at[slot, pc], slot, pc, d).start()

    def relay_y(n):
        pc = piece_of(n)
        for d in range(ways):
            slot = lax.rem(a + ways - d, ways) * group + (g + 2) % group
            kv_wait(slot, pc)
            to_mate(kvbuf.at[slot, pc], slot, pc, ways + d).start()

    for c in loads:
        c.wait()

    def front(n, carry):
        pc = piece_of(n)

        @pl.when(n >= 2)
        def _():
            tok_copy(n - 2).wait_recv()

        x = toks[n].astype(jnp.float32)
        x = x * lax.rsqrt(jnp.mean(x * x, axis=-1, keepdims=True) + 1e-06) * gain_ref[...]
        nrm[...] = x.astype(jnp.bfloat16)

        def product(k, c):
            raw[k] = jnp.dot(nrm[...], w[k], preferred_element_type=jnp.float32)
            return c

        lax.fori_loop(0, 5, product, 0)

        def rounded(k, h):
            return raw[k, :, h * 2 * hd:(h + 1) * 2 * hd].astype(jnp.bfloat16).astype(jnp.float32)

        for h in range(ways):
            qs[pc, h] = prepared(rounded(0, h).T, hd ** -0.5, pc).astype(jnp.bfloat16)
            kvs[pc, h, :prow] = prepared(rounded(1, h).T, 1.0, pc).T.astype(jnp.bfloat16)
            kvs[pc, h, prow:] = raw[2, :, h * vdim:(h + 1) * vdim].astype(jnp.bfloat16).astype(jnp.float32).T.astype(
                jnp.bfloat16)
        for d in range(1, ways):
            kv_z(pc, d).start()
        to_across(kvs.at[pc, a], s, pc, 0).start()
        to_mate(kvs.at[pc, a], s, pc, 0).start()
        for d in range(1, ways):
            q_z(pc, d).start()

        @pl.when(stays)
        def _():
            qbuf[a, pc] = qs[pc, a]

        @pl.when(jnp.logical_not(stays))
        def _():
            q_z(pc, 0).start()

        kvbuf[s, pc] = kvs[pc, a]
        ga = raw[3].astype(jnp.bfloat16).astype(jnp.float32)
        gg = raw[4].astype(jnp.bfloat16).astype(jnp.float32)
        gated = (ga * jax.nn.sigmoid(gg)).astype(jnp.bfloat16)
        gext[pl.ds(pl.multiple_of(32 + pc * prow, 32), prow)] = gated.astype(jnp.float32)

        @pl.when(pc == PIECES - 1)
        def _():
            glast[...] = gated[prow - 32:]

        @pl.when(n >= 1)
        def _():
            relay_z(n - 1)

        @pl.when(n >= 2)
        def _():
            relay_y(n - 2)

        return carry

    halo_out = remote(glast, halo, halo_send.at[0], halo_recv.at[0], lax.rem(s + 1, sp), t)
    lax.fori_loop(0, PIECES, front, 0)

    @pl.when(s < sp - 1)
    def _():
        halo_out.start()

    @pl.when(s > 0)
    def _():
        halo_out.wait_recv()
        gext[0:32] = halo[...].astype(jnp.float32)

    @pl.when(s == 0)
    def _():
        gext[0:32] = jnp.zeros((32, cch), jnp.float32)

    def st_copy(r):
        return remote(st.at[r], str_.at[r], st_send.at[r], st_recv.at[r], s, other)

    def convolve(r, carry):
        plain = jnp.zeros((prow, 128), jnp.float32)
        square = jnp.zeros((prow, 128), jnp.float32)
        for c in range(cch // 128):
            lanes = slice(c * 128, (c + 1) * 128)
            window = gext[pl.ds(pl.multiple_of(r * prow, prow), prow + 32), lanes]
            total = jnp.zeros((prow, 128), jnp.float32)
            for k in range(8):
                turned = window if k == 0 else pltpu.roll(window, prow + 32 - k, 0)
                for j in range(taps):
                    place = 32 - (taps - 1) + j
                    if place % 8 == k:
                        total = total + taps_ref[j:j + 1, lanes] * turned[place - k:place - k + prow]
            conv[r, :, lanes] = total
            plain = plain + total
            square = square + total * total
        st[r, 0:1] = jnp.sum(plain.T, axis=0, keepdims=True)
        st[r, 1:2] = jnp.sum(square.T, axis=0, keepdims=True)
        st_copy(r).start()
        return carry

    lax.fori_loop(0, PIECES, convolve, 0)
    relay_z(PIECES - 1)

    def cv_copy(j):
        return remote(cvo.at[other * 2 + j], cvr.at[j], cv_send.at[j], cv_recv.at[j], s, other)

    def normalize(r, carry):
        st_copy(r).wait_recv()
        both = st[r] + str_[r]
        mean = both[0:1] / channels
        scale = lax.rsqrt(both[1:2] / channels - mean * mean + 1e-05)
        mean = jnp.broadcast_to(mean, (128, prow)).T
        scale = jnp.broadcast_to(scale, (128, prow)).T
        for c in range(cch // 128):
            lanes = slice(c * 128, (c + 1) * 128)
            y = (conv[r, :, lanes] - mean) * scale * cgain_ref[:, lanes] + cshift_ref[:, lanes]
            cvo[r, :, lanes] = (y * jax.nn.sigmoid(y)).astype(jnp.bfloat16)
        return carry

    lax.fori_loop(0, PIECES, normalize, 0)
    for j in range(2):
        cv_copy(j).start()
    relay_y(PIECES - 2)
    relay_y(PIECES - 1)
    out_load.wait()
    for j in range(2):
        cv_copy(j).wait_recv()
    own = 2 * prow
    wide = wo.shape[1]
    step = wide // 4
    top = ways * tp * vdim

    def conv_part(n, carry):
        cols = pl.ds(pl.multiple_of(n * step, step), step)
        mine = wo[pl.ds(pl.multiple_of(top + t * cch, cch), cch), cols]
        theirs = wo[pl.ds(pl.multiple_of(top + other * cch, cch), cch), cols]
        macc[:, cols] = jnp.dot(
            cvo[pl.ds(t * 2, 2)].reshape(own, cch), mine, preferred_element_type=jnp.float32) + jnp.dot(
            cvr[...].reshape(own, cch), theirs, preferred_element_type=jnp.float32)
        return carry

    lax.fori_loop(0, 4, conv_part, 0)

    def mate_wait(pc, carry):
        for b in range(ways):
            for e in range(2):
                slot = b * group + (mate - a * group + 2 * e) % group
                kv_wait(slot, pc)
        return carry

    lax.fori_loop(0, PIECES, mate_wait, 0)

    def q_wait(i, pc):
        remote(qs.at[pc, 0], qbuf.at[i, pc], q_send.at[0, 0], q_recv.at[i, pc], s, other).wait_recv()

    def q_waits(i, carry):
        here = jnp.logical_and(i == a, stays)

        @pl.when(jnp.logical_not(here))
        def _():
            for pc in range(PIECES):
                q_wait(i, pc)

        return carry

    lax.fori_loop(0, ways, q_waits, 0)

    lam = lam_ref[a]
    head = t * ways + a

    def ao_copy(i, hf, slot):
        return remote(aos.at[i, hf], ao.at[slot], ao_send.at[i, hf], ao_recv.at[slot], i * group + turn(i), hf)

    def lt_copy(i, slot):
        return remote(lts.at[i], lor.at[slot], lt_send.at[i], lt_recv.at[slot], i * group + turn(i), t)

    def attend(n, carry):
        i = lax.rem(a + 1 + n, ways)
        chunk = i * group + turn(i)
        queries = [
            jnp.concatenate([qbuf[i, pc, m * hd:(m + 1) * hd, :] for pc in range(PIECES)], axis=1) for m in range(2)]

        def score(j, ref):
            for m in range(2):
                keys = kvbuf[j, :, :prow, m * hd:(m + 1) * hd].reshape(rows, hd)
                ref[m] = jnp.dot(keys, queries[m], preferred_element_type=jnp.float32)

        def absorb(j, ref, tops, masked=False):
            vb = jnp.concatenate([kvbuf[j, pc, prow:] for pc in range(PIECES)], axis=1)
            vb = jnp.concatenate([vb, jnp.ones((16, rows), jnp.bfloat16)], axis=0)
            out = []
            for m in range(2):
                sc = ref[m]
                if masked:
                    kp = lax.broadcasted_iota(jnp.int32, sc.shape, 0)
                    qp = lax.broadcasted_iota(jnp.int32, sc.shape, 1)
                    sc = jnp.where(kp <= qp, sc, NEG)
                new = jnp.maximum(tops[m], jnp.max(sc, axis=0, keepdims=True))
                p = jnp.exp(sc - new)
                f = jnp.exp(tops[m] - new)
                acc[m] = acc[m] * f + jnp.dot(vb, p.astype(jnp.bfloat16), preferred_element_type=jnp.float32)
                out.append(new)
            return tuple(out)

        acc[...] = jnp.zeros_like(acc)
        one = jnp.full((1, rows), NEG, jnp.float32)
        score(chunk, sa)
        score(0, sb)
        tops = absorb(chunk, sa, (one, one), True)

        def pair(j, tops):
            score(2 * j + 1, sa)
            tops = absorb(2 * j, sb, tops)
            score(2 * j + 2, sb)
            return absorb(2 * j + 1, sa, tops)

        tops = lax.fori_loop(0, chunk // 2, pair, tops)
        tops = lax.cond(chunk % 2 == 1, lambda v: absorb(chunk - 1, sb, v), lambda v: v, tops)
        l0 = acc[0, vdim:vdim + 1]
        l1 = acc[1, vdim:vdim + 1]
        heads = acc[0, :vdim] / l0 - lam * acc[1, :vdim] / l1
        heads = heads * lax.rsqrt(jnp.mean(heads * heads, axis=0, keepdims=True) + 1e-06)
        heads = (heads.T * hgain_ref[...]).astype(jnp.bfloat16)
        lts[i, 0:1] = tops[0] + jnp.log(l0)
        lts[i, 1:2] = tops[1] + jnp.log(l1)
        here = jnp.logical_and(i == a, stays)
        for hf in range(2):
            aos[i, hf] = heads[hf * own:(hf + 1) * own]
            mine = jnp.logical_and(here, t == hf)

            @pl.when(mine)
            def _():
                ao[head] = heads[hf * own:(hf + 1) * own]

            @pl.when(jnp.logical_not(mine))
            def _():
                ao_copy(i, hf, head).start()

        @pl.when(here)
        def _():
            lor[a] = lts[i]

        @pl.when(jnp.logical_not(here))
        def _():
            lt_copy(i, a).start()

        return carry

    lax.fori_loop(0, ways, attend, 0)

    def gather(h, carry):
        b = h % ways
        local = jnp.logical_and(jnp.logical_and(b == a, h // ways == t), stays)

        @pl.when(jnp.logical_not(local))
        def _():
            remote(aos.at[0, 0], ao.at[h], ao_send.at[0, 0], ao_recv.at[h], s, other).wait_recv()

        return carry

    lax.fori_loop(0, ways * tp, gather, 0)

    def att_part(n, carry):
        cols = pl.ds(pl.multiple_of(n * step, step), step)
        left = jnp.concatenate([ao[h] for h in range(ways * tp)], axis=1)
        mixed_ref[:, cols] = (
            macc[:, cols] + jnp.dot(left, wo[:top, cols], preferred_element_type=jnp.float32)).astype(jnp.bfloat16)
        return carry

    lax.fori_loop(0, 4, att_part, 0)

    for b in range(ways):
        local = jnp.logical_and(b == a, stays)

        @pl.when(jnp.logical_not(local))
        def _():
            remote(lts.at[0], lor.at[b], lt_send.at[0], lt_recv.at[b], s, other).wait_recv()

        for m in range(2):
            lo_ref[m, b:b + 1] = lor[b, m:m + 1]

    for j in range(2):
        tok_copy(j).wait_send()
        cv_copy(j).wait_send()

    def drain(pc, carry):
        for d in range(1, ways):
            kv_z(pc, d).wait_send()
            q_z(pc, d).wait_send()

        @pl.when(jnp.logical_not(stays))
        def _():
            q_z(pc, 0).wait_send()

        for d in range(ways):
            to_across(kvs.at[pc, 0], s, pc, d).wait_send()
        for d in range(2 * ways):
            to_mate(kvs.at[pc, 0], s, pc, d).wait_send()
        st_copy(pc).wait_send()
        return carry

    lax.fori_loop(0, PIECES, drain, 0)

    @pl.when(s < sp - 1)
    def _():
        halo_out.wait_send()

    def drain_out(i, carry):
        here = jnp.logical_and(i == a, stays)
        for hf in range(2):
            @pl.when(jnp.logical_not(jnp.logical_and(here, t == hf)))
            def _():
                ao_copy(i, hf, head).wait_send()

        @pl.when(jnp.logical_not(here))
        def _():
            lt_copy(i, a).wait_send()

        return carry

    lax.fori_loop(0, ways, drain_out, 0)


def whole_layer(
    sp, tp, tokens, norm_gain, query_weight, key_weight, value_weight, glu_value_weight, glu_gate_weight,
    qk_gain, mix_lambda, head_gain, conv_kernel, channel_gain, channel_shift, output_weight,
):
    ways = mix_lambda.shape[0]
    group = sp // ways
    own, width = tokens.shape
    rows = own * tp
    prow = rows // PIECES
    hd = qk_gain.shape[1]
    half = hd // 2
    vdim = head_gain.shape[0]
    taps, cch = conv_kernel.shape
    me = lax.axis_index("sp")
    order = jnp.arange(rows, dtype=jnp.int32).reshape(PIECES, 1, prow)
    positions = (me * rows + order).astype(jnp.float32)
    inverse = 10000.0 ** (-jnp.arange(0, half, dtype=jnp.float32) * 2.0 / hd)
    angles = positions * inverse[None, :, None]
    cosine, sine = jnp.cos(angles)[:, None], jnp.sin(angles)[:, None]
    first, second = qk_gain[None, :, :half, None], qk_gain[None, :, half:, None]
    tab = jnp.stack([first * cosine, second * sine, second * cosine, first * sine], axis=2)
    f32, bf16 = jnp.float32, jnp.bfloat16
    any_ = pl.BlockSpec(memory_space=pl.ANY)
    vm = pl.BlockSpec(memory_space=pltpu.VMEM)
    sm = pl.BlockSpec(memory_space=pltpu.SMEM)
    dma = pltpu.SemaphoreType.DMA
    return pl.pallas_call(
        lambda *refs: layer_kernel((ways, group, tp, taps), *refs),
        out_shape=(
            jax.ShapeDtypeStruct((own, output_weight.shape[1]), bf16), jax.ShapeDtypeStruct((2, ways, rows), f32)),
        in_specs=[any_, vm, any_, any_, any_, any_, any_, any_, sm, vm, vm, vm, vm, any_],
        out_specs=(vm, vm),
        scratch_shapes=[
            pltpu.VMEM((PIECES, prow, width), bf16),
            pltpu.VMEM((5,) + query_weight.shape, bf16),
            pltpu.VMEM(tab.shape, f32),
            pltpu.VMEM(output_weight.shape, bf16),
            pltpu.VMEM((prow, width), bf16),
            pltpu.VMEM((5, prow, cch), f32),
            pltpu.VMEM((PIECES, ways, 2 * hd, prow), bf16),
            pltpu.VMEM((PIECES, ways, prow + vdim, 2 * hd), bf16),
            pltpu.VMEM((ways, PIECES, 2 * hd, prow), bf16),
            pltpu.VMEM((sp, PIECES, prow + vdim, 2 * hd), bf16),
            pltpu.VMEM((32 + rows, cch), f32),
            pltpu.VMEM((32, cch), bf16),
            pltpu.VMEM((32, cch), bf16),
            pltpu.VMEM((PIECES, prow, cch), f32),
            pltpu.VMEM((PIECES, prow, cch), bf16),
            pltpu.VMEM((2, prow, cch), bf16),
            pltpu.VMEM((PIECES, 2, prow), f32),
            pltpu.VMEM((PIECES, 2, prow), f32),
            pltpu.VMEM((own, output_weight.shape[1]), f32),
            pltpu.VMEM((2, rows, rows), f32),
            pltpu.VMEM((2, rows, rows), f32),
            pltpu.VMEM((2, vdim + 16, rows), f32),
            pltpu.VMEM((ways, 2, own, vdim), bf16),
            pltpu.VMEM((ways * tp, own, vdim), bf16),
            pltpu.VMEM((ways, 2, rows), f32),
            pltpu.VMEM((ways, 2, rows), f32),
            dma((9,)), dma((2,)), dma((2,)),
            dma((PIECES, ways)), dma((ways, PIECES)), dma((PIECES, ways - 1)), dma((sp, PIECES)),
            dma((ways, PIECES)), dma((2 * ways, PIECES)), dma((1,)), dma((1,)),
            dma((PIECES,)), dma((PIECES,)), dma((2,)), dma((2,)),
            dma((ways, 2)), dma((ways * tp,)), dma((ways,)), dma((ways,)),
        ],
        compiler_params=pltpu.CompilerParams(
            collective_id=3, has_side_effects=True, vmem_limit_bytes=67043328),
        name="layer",
    )(
        tokens, norm_gain.reshape(1, width), query_weight, key_weight, value_weight, glu_value_weight, glu_gate_weight,
        tab, mix_lambda, head_gain.reshape(1, vdim), conv_kernel, channel_gain.reshape(1, cch),
        channel_shift.reshape(1, cch), output_weight)


def per_device(
    tokens, norm_gain, query_weight, key_weight, value_weight, glu_value_weight, glu_gate_weight,
    qk_gain, mix_lambda, head_gain, conv_kernel, channel_gain, channel_shift, output_weight,
):
    head_size = qk_gain.shape[1]
    heads_here = mix_lambda.shape[0]
    value_size = head_gain.shape[0]
    kernel_len = conv_kernel.shape[0]
    conv_here = conv_kernel.shape[1]
    width = tokens.shape[1]
    sp = lax.axis_size("sp")
    tp = lax.axis_size("tp")
    me = lax.axis_index("sp")
    t = lax.axis_index("tp")
    ways = heads_here
    group = sp // ways
    own = tokens.shape[0]
    rows = own * tp
    if tp == 2 and ways * group == sp and group == 4 and ways % 2 == 0 and own == 256 and head_size == 64 and value_size == 128:
        return whole_layer(
            sp, tp, tokens, norm_gain, query_weight, key_weight, value_weight, glu_value_weight, glu_gate_weight,
            qk_gain, mix_lambda, head_gain, conv_kernel, channel_gain, channel_shift, output_weight)

    def norm(piece):
        inputs = piece.astype(jnp.float32)
        return (
            inputs * lax.rsqrt(jnp.mean(inputs * inputs, axis=-1, keepdims=True) + 1e-06) * norm_gain
        ).astype(jnp.bfloat16)

    others = [tokens] + [
        lax.ppermute(tokens, "tp", [(i, (i - d) % tp) for i in range(tp)]) for d in range(1, tp)
    ]
    if tp == 2:
        other = others[1]
        normed = norm(jnp.concatenate([jnp.where(t == 0, tokens, other), jnp.where(t == 0, other, tokens)], axis=0))
    else:
        stacked = jnp.stack(others)
        normed = norm(jnp.concatenate(
            [lax.dynamic_index_in_dim(stacked, (j - t) % tp, 0, keepdims=False) for j in range(tp)], axis=0))

    def turned(matrix):
        return lax.dot_general(matrix, normed, (((0,), (1,)), ((), ())), preferred_element_type=jnp.float32).astype(jnp.bfloat16)

    def plain(matrix):
        return jnp.dot(normed, matrix, preferred_element_type=jnp.float32).astype(jnp.bfloat16)

    positions = (me * rows + jnp.arange(rows, dtype=jnp.int32)).astype(jnp.float32)
    inverse = 10000.0 ** (-jnp.arange(0, head_size // 2, dtype=jnp.float32) * 2.0 / head_size)
    angles = positions[None, :] * inverse[:, None]
    cosine, sine = jnp.cos(angles)[None, None], jnp.sin(angles)[None, None]
    shape = (heads_here, 2, head_size, rows)
    rq = prepare_t(turned(query_weight).reshape(shape), qk_gain, cosine, sine) * jnp.bfloat16(head_size ** -0.5)
    rk = prepare_t(turned(key_weight).reshape(shape), qk_gain, cosine, sine)
    qt = rq.reshape(heads_here, 2 * head_size, rows)
    kk = jnp.transpose(rk.reshape(heads_here, 2 * head_size, rows), (0, 2, 1))
    vt = turned(value_weight).reshape(heads_here, value_size, rows)
    kv = jnp.concatenate([kk, vt.reshape(heads_here, value_size, rows // 128, 128).transpose(0, 2, 1, 3).reshape(heads_here, -1, 128)], axis=1)
    qall, kvall = spread(qt, kv, ways, group)

    glu_a, glu_g = plain(glu_value_weight), plain(glu_gate_weight)
    gated = (glu_a.astype(jnp.float32) * jax.nn.sigmoid(glu_g.astype(jnp.float32))).astype(jnp.bfloat16)
    earlier = from_behind(gated[rows - (kernel_len - 1):], "sp", 1)
    extended = jnp.concatenate([earlier, gated], axis=0).astype(jnp.float32)
    convolved = jnp.zeros((rows, conv_here), jnp.float32)
    for step in range(kernel_len):
        convolved = convolved + conv_kernel[step][None, :] * extended[step:step + rows]
    plain_sum, square_sum = lax.psum(
        (jnp.sum(convolved, axis=1), jnp.sum(convolved * convolved, axis=1)), "tp"
    )
    channels = conv_here * tp
    middle = (plain_sum / channels)[:, None]
    spread_ = (square_sum / channels)[:, None] - middle * middle
    conv_out = jax.nn.silu(
        (convolved - middle) * lax.rsqrt(spread_ + 1e-05) * channel_gain + channel_shift
    ).astype(jnp.bfloat16)

    place = (me % group).astype(jnp.int32).reshape(1)
    lam = lax.dynamic_slice(mix_lambda, (me // group,), (1,))
    att, lt = attention(place, lam, head_gain, qall, kvall)
    ao, lo, co = collect(
        att.reshape(ways, tp, own, value_size), lt, conv_out.reshape(tp, own, conv_here), ways, group, tp)
    heads = ways * tp
    merged = jnp.concatenate([
        jnp.transpose(ao, (1, 0, 2)).reshape(own, heads * value_size),
        jnp.transpose(co, (1, 0, 2)).reshape(own, channels)], axis=1)
    mixed = jnp.dot(merged, output_weight, preferred_element_type=jnp.float32).astype(jnp.bfloat16)
    return (mixed, jnp.transpose(lo, (1, 0, 2)))


def solution(mesh):
    placed = (
        P(("sp", "tp"), None), P(), P(None, "tp"), P(None, "tp"), P(None, "tp"), P(None, "tp"), P(None, "tp"),
        P(), P("tp"), P(), P(None, "tp"), P("tp"), P("tp"), P(),
    )
    return jax.shard_map(
        per_device,
        mesh=mesh,
        in_specs=placed,
        out_specs=(P(("sp", "tp"), None), P(None, "tp", "sp")),
        check_vma=False,
    )
```

```python
import math

import jax
import jax.numpy as jnp
from jax import lax
from jax.experimental import pallas as pl
from jax.experimental.pallas import tpu as pltpu
from jax.sharding import PartitionSpec as P

MESH = pl.DeviceIdType.MESH
NEG = -1e30


def from_behind(value, axis, steps):
    count = lax.axis_size(axis)
    leading, last = (max(0, -steps), min(count, count - steps))
    return lax.ppermute(value, axis, [(source, source + steps) for source in range(leading, last)])


def flipped(g, a, group):
    if group % 2:
        return g
    return jnp.where(a % 2 == 0, g, group - 1 - g)


def spread_kernel(ways, group, q_ref, kv_ref, qo_ref, kvo_ref, qsend, qrecv, ksend, kfwd, krelay, krecv, local):
    me = lax.axis_index("sp")
    a = me // group
    g = me % group
    cores = 2 if group % 2 == 0 else 1
    half = group // cores
    mate = a * group + (g + 1 - 2 * (g % 2)) if cores == 2 else me

    def same(d):
        return (g + d * cores) % group

    peers = [lax.rem(a + d, ways) * group + g for d in range(1, ways)]
    peers += [a * group + same(d) for d in range(1, half)]
    if cores == 2:
        peers.append(mate)
        peers += [lax.rem(a + d, ways) * group + group - 1 - g for d in range(ways)]
    barrier = pltpu.get_barrier_semaphore()
    for peer in peers:
        pl.semaphore_signal(barrier, inc=1, device_id={"sp": peer}, device_id_type=MESH)
    pl.semaphore_wait(barrier, len(peers))

    def kv_copy(src, slot, send, peer):
        return pltpu.make_async_remote_copy(
            src_ref=src, dst_ref=kvo_ref.at[slot], send_sem=send, recv_sem=krecv.at[slot],
            device_id={"sp": peer}, device_id_type=MESH)

    sends = []
    keep = pltpu.make_async_copy(kv_ref.at[a], kvo_ref.at[me], local.at[0])
    keep_q = pltpu.make_async_copy(q_ref.at[a], qo_ref.at[a], local.at[1])
    keep.start()

    def q_copy(h, slot, d):
        return pltpu.make_async_remote_copy(
            src_ref=q_ref.at[h], dst_ref=qo_ref.at[slot], send_sem=qsend.at[d], recv_sem=qrecv.at[slot],
            device_id={"sp": h * group + flipped(g, a, group)}, device_id_type=MESH)

    stays = a % 2 == 0 if cores == 2 else a >= 0

    @pl.when(stays)
    def _():
        keep_q.start()
    order = list(range(1, ways))
    for d in order:
        h = lax.rem(a + d, ways)
        c = kv_copy(kv_ref.at[h], me, ksend.at[d - 1], h * group + g)
        c.start()
        sends.append(c)

    def forward(d):
        src_a = lax.rem(a + ways - d, ways)
        slot = src_a * group + g
        if d:
            kv_copy(kvo_ref.at[slot], slot, ksend.at[d - 1], me).wait_recv()
            src = kvo_ref.at[slot]
        else:
            src = kv_ref.at[a]
        n = 0
        for e in range(1, half):
            c = kv_copy(src, slot, kfwd.at[d, n], a * group + same(e))
            c.start()
            sends.append(c)
            n += 1
        if cores == 2:
            c = kv_copy(src, slot, kfwd.at[d, n], mate)
            c.start()
            sends.append(c)

    def relay(d):
        src_a = lax.rem(a + ways - d, ways)
        for e in range(1, half):
            slot = src_a * group + same(e)
            kv_copy(kvo_ref.at[slot], slot, krelay.at[d, e - 1], mate).wait_recv()
            if cores == 2:
                c = kv_copy(kvo_ref.at[slot], slot, krelay.at[d, e - 1], mate)
                c.start()
                sends.append(c)

    forward(0)
    for d in order:
        c = q_copy(lax.rem(a + d, ways), a, d)
        c.start()
        sends.append(c)
    if cores == 2:
        @pl.when(jnp.logical_not(stays))
        def _():
            q_copy(a, a, 0).start()
    for d in range(1, ways):
        forward(d)
        relay(d - 1)
    relay(ways - 1)
    if cores == 2:
        for d in range(ways):
            src_a = lax.rem(a + ways - d, ways)
            for e in range(half):
                slot = src_a * group + (g + 1 - 2 * (g % 2) + e * cores) % group
                kv_copy(kvo_ref.at[slot], slot, krelay.at[0, 0], mate).wait_recv()
    for d in range(1, ways):
        src_a = lax.rem(a + ways - d, ways)
        q_copy(a, src_a, d).wait_recv()
    for c in sends:
        c.wait_send()
    keep.wait()

    @pl.when(stays)
    def _():
        keep_q.wait()

    if cores == 2:
        @pl.when(jnp.logical_not(stays))
        def _():
            q_copy(a, a, 0).wait()


def spread(q, kv, ways, group):
    cores = 2 if group % 2 == 0 else 1
    half = group // cores
    any_ = pl.BlockSpec(memory_space=pl.ANY)
    n = max(ways - 1, 1)
    return pl.pallas_call(
        lambda *refs: spread_kernel(ways, group, *refs),
        out_shape=(
            jax.ShapeDtypeStruct(q.shape, q.dtype),
            jax.ShapeDtypeStruct((ways * group,) + kv.shape[1:], kv.dtype),
        ),
        in_specs=[any_, any_],
        out_specs=(any_, any_),
        scratch_shapes=[
            pltpu.SemaphoreType.DMA((ways,)),
            pltpu.SemaphoreType.DMA((ways,)),
            pltpu.SemaphoreType.DMA((n,)),
            pltpu.SemaphoreType.DMA((ways, half)),
            pltpu.SemaphoreType.DMA((ways, max(half - 1, 1))),
            pltpu.SemaphoreType.DMA((ways * group,)),
            pltpu.SemaphoreType.DMA((2,)),
        ],
        compiler_params=pltpu.CompilerParams(collective_id=1, has_side_effects=True),
        name="spread",
    )(q, kv)


def collect_kernel(ways, group, tp, att_ref, lt_ref, conv_ref, ao_ref, lo_ref, co_ref, asend, arecv, lsend, lrecv, csend, crecv, local):
    me = lax.axis_index("sp")
    t = lax.axis_index("tp")
    a = me // group
    g = me % group
    vdim = att_ref.shape[-1]
    cch = conv_ref.shape[-1]

    def coords(i):
        dt, da = i % tp, i // tp
        return lax.rem(a + da, ways), lax.rem(t + dt, tp)

    total = ways * tp
    both = group % 2 == 0
    barrier = pltpu.get_barrier_semaphore()
    for i in range(total):
        pa, pt = coords(i)
        if i:
            pl.semaphore_signal(barrier, inc=1, device_id={"sp": pa * group + g, "tp": pt}, device_id_type=MESH)
        if both:
            pl.semaphore_signal(
                barrier, inc=1, device_id={"sp": pa * group + group - 1 - g, "tp": pt}, device_id_type=MESH)
    pl.semaphore_wait(barrier, 2 * total - 1 if both else total - 1)

    head = t * ways + a

    def att_copy(i, slot):
        pa, pt = coords(i)
        return pltpu.make_async_remote_copy(
            src_ref=att_ref.at[pa, pt], dst_ref=ao_ref.at[slot], send_sem=asend.at[i], recv_sem=arecv.at[slot],
            device_id={"sp": pa * group + flipped(g, pa, group), "tp": pt}, device_id_type=MESH)

    def lt_copy(i, slot):
        pa = lax.rem(a + i, ways)
        return pltpu.make_async_remote_copy(
            src_ref=lt_ref.at[pa], dst_ref=lo_ref.at[slot], send_sem=lsend.at[i], recv_sem=lrecv.at[slot],
            device_id={"sp": pa * group + flipped(g, pa, group), "tp": t}, device_id_type=MESH)

    stays = a % 2 == 0 if both else a >= 0
    sends = []
    for i in range(total - 1, 0, -1):
        c = att_copy(i, head)
        c.start()
        sends.append(c)
    for i in range(1, tp):
        pa, pt = coords(i)
        c = pltpu.make_async_remote_copy(
            src_ref=conv_ref.at[pt], dst_ref=co_ref.at[t],
            send_sem=csend.at[i], recv_sem=crecv.at[t],
            device_id={"sp": me, "tp": pt}, device_id_type=MESH)
        c.start()
        sends.append(c)
    for i in range(1, ways):
        c = lt_copy(i, a)
        c.start()
        sends.append(c)
    keep = pltpu.make_async_copy(conv_ref.at[t], co_ref.at[t], local.at[1])
    keep.start()
    mine = [
        pltpu.make_async_copy(att_ref.at[a, t], ao_ref.at[head], local.at[0]),
        pltpu.make_async_copy(lt_ref.at[a], lo_ref.at[a], local.at[2]),
    ]

    @pl.when(stays)
    def _():
        for c in mine:
            c.start()

    if both:
        @pl.when(jnp.logical_not(stays))
        def _():
            att_copy(0, head).start()
            lt_copy(0, a).start()
    for i in range(1, total):
        pa, pt = coords(i)
        att_copy(i, pt * ways + pa).wait_recv()
    for i in range(1, tp):
        pa, pt = coords(i)
        pltpu.make_async_remote_copy(
            src_ref=conv_ref.at[t], dst_ref=co_ref.at[pt],
            send_sem=csend.at[i], recv_sem=crecv.at[pt],
            device_id={"sp": me, "tp": pt}, device_id_type=MESH).wait_recv()
    for i in range(1, ways):
        lt_copy(i, lax.rem(a + i, ways)).wait_recv()
    for c in sends:
        c.wait_send()
    keep.wait()

    @pl.when(stays)
    def _():
        for c in mine:
            c.wait()

    if both:
        @pl.when(jnp.logical_not(stays))
        def _():
            att_copy(0, head).wait()
            lt_copy(0, a).wait()


def collect(att, lt, conv, ways, group, tp):
    any_ = pl.BlockSpec(memory_space=pl.ANY)
    rows, vdim = att.shape[2:]
    total = ways * tp
    return pl.pallas_call(
        lambda *refs: collect_kernel(ways, group, tp, *refs),
        out_shape=(
            jax.ShapeDtypeStruct((total, rows, vdim), att.dtype),
            jax.ShapeDtypeStruct(lt.shape, lt.dtype),
            jax.ShapeDtypeStruct(conv.shape, conv.dtype),
        ),
        in_specs=[any_] * 3,
        out_specs=(any_,) * 3,
        scratch_shapes=[
            pltpu.SemaphoreType.DMA((total,)),
            pltpu.SemaphoreType.DMA((total,)),
            pltpu.SemaphoreType.DMA((ways,)),
            pltpu.SemaphoreType.DMA((ways,)),
            pltpu.SemaphoreType.DMA((tp,)),
            pltpu.SemaphoreType.DMA((tp,)),
            pltpu.SemaphoreType.DMA((3,)),
        ],
        compiler_params=pltpu.CompilerParams(collective_id=2, has_side_effects=True),
        name="collect",
    )(att, lt, conv)


def attention(place, lam, head_gain, qt, kv, tile=512):
    ways, qdim, rows = qt.shape
    hd = qdim // 2
    blocks = kv.shape[0]
    vdim = head_gain.shape[0]
    group = blocks // ways
    tile = math.gcd(tile, rows)
    tiles = rows // tile
    def kernel(place_ref, lam_ref, gain_ref, q_ref, kv_ref, o_ref, lt_ref, sa, sb, acc_ref):
        i = pl.program_id(0); s = pl.program_id(1)
        chunk = i * group + flipped(place_ref[0], i, group)
        qs = [q_ref[0, m * hd:(m + 1) * hd, :] for m in range(2)]
        def score(j, ref):
            for m in range(2):
                ref[m] = jnp.dot(kv_ref[j, :rows, m * hd:(m + 1) * hd], qs[m], preferred_element_type=jnp.float32)
        def absorb(j, ref, tops, masked=False):
            vb = jnp.concatenate([kv_ref[j, rows + b * vdim:rows + (b + 1) * vdim] for b in range(rows // 128)], axis=1)
            vb = jnp.concatenate([vb, jnp.ones((16, rows), jnp.bfloat16)], axis=0)
            out=[]
            for m in range(2):
                sc = ref[m]
                if masked:
                    kp = lax.broadcasted_iota(jnp.int32, sc.shape, 0)
                    qp = lax.broadcasted_iota(jnp.int32, sc.shape, 1) + s * tile
                    sc = jnp.where(kp <= qp, sc, NEG)
                new = jnp.maximum(tops[m], jnp.max(sc, axis=0, keepdims=True))
                p = jnp.exp(sc - new)
                f = jnp.exp(tops[m] - new)
                acc_ref[m] = acc_ref[m] * f + jnp.dot(vb, p.astype(jnp.bfloat16), preferred_element_type=jnp.float32)
                out.append(new)
            return tuple(out)
        acc_ref[...] = jnp.zeros_like(acc_ref)
        one = jnp.full((1, tile), NEG, jnp.float32)
        score(chunk, sa)
        score(0, sb)
        tops = absorb(chunk, sa, (one, one), True)

        def pair(j, tops):
            score(2 * j + 1, sa)
            tops = absorb(2 * j, sb, tops)
            score(2 * j + 2, sb)
            return absorb(2 * j + 1, sa, tops)

        tops = lax.fori_loop(0, chunk // 2, pair, tops)
        tops = lax.cond(chunk % 2 == 1, lambda t: absorb(chunk - 1, sb, t), lambda t: t, tops)
        a0=acc_ref[0]; a1=acc_ref[1]
        t0,t1=tops
        l0=a0[vdim:vdim+1]; l1=a1[vdim:vdim+1]; a0=a0[:vdim]; a1=a1[:vdim]
        heads = a0 / l0 - lam_ref[0] * a1 / l1
        heads = heads * lax.rsqrt(jnp.mean(heads * heads, axis=0, keepdims=True) + 1e-06) * gain_ref[...]
        o_ref[0] = heads.T.astype(jnp.bfloat16)
        lt_ref[0, 0:1, :] = t0 + jnp.log(l0)
        lt_ref[0, 1:2, :] = t1 + jnp.log(l1)
    smem = pl.BlockSpec(memory_space=pltpu.SMEM)
    return pl.pallas_call(kernel, grid=(ways, tiles),
        out_shape=(jax.ShapeDtypeStruct((ways, rows, vdim), jnp.bfloat16), jax.ShapeDtypeStruct((ways, 2, rows), jnp.float32)),
        in_specs=[smem, smem, pl.BlockSpec((vdim, 1), lambda i, s: (0, 0)), pl.BlockSpec((1, qdim, tile), lambda i, s: (i, 0, s)), pl.BlockSpec(kv.shape, lambda i, s: (0, 0, 0))],
        out_specs=(pl.BlockSpec((1, tile, vdim), lambda i, s: (i, s, 0)), pl.BlockSpec((1, 2, tile), lambda i, s: (i, 0, s))),
        scratch_shapes=[pltpu.VMEM((2,rows,tile),jnp.float32),pltpu.VMEM((2,rows,tile),jnp.float32),pltpu.VMEM((2,vdim+16,tile),jnp.float32)],
        compiler_params=pltpu.CompilerParams(vmem_limit_bytes=58 << 20), name="attend")(place, lam, head_gain.reshape(-1, 1), qt, kv)


def prepare_t(raw, qk_gain, cosine, sine):
    values = raw.astype(jnp.float32)
    values = values * lax.rsqrt(jnp.mean(values * values, axis=2, keepdims=True) + 1e-06)
    values = values * qk_gain[None, :, :, None]
    half = raw.shape[2] // 2
    first, second = values[:, :, :half], values[:, :, half:]
    return jnp.concatenate(
        [first * cosine - second * sine, second * cosine + first * sine], axis=2
    ).astype(jnp.bfloat16)

PIECES = 4


def balanced(ways, group):
    counts = {
        sum((i * group + (g if i % 2 == 0 else group - 1 - g)) // 2 for i in range(ways)) for g in range(group)}
    return counts.pop() if len(counts) == 1 else 1


def layer_kernel(
    sizes, tokens_ref, gain_in, wq_ref, wk_ref, wv_ref, wa_ref, wg_ref, qkg_in, lam_in, hgain_in, taps_in,
    cgain_in, cshift_in, wo_ref, mixed_ref, lo_ref,
    gain_ref, qkg_ref, lam_ref, hgain_ref, taps_ref, cgain_ref, cshift_ref,
    toks, w, tab, wo, nrm, raw, qs, kvs, qbuf, kvbuf, gext, glast, halo, conv, cvo, cvr, st, str_, macc,
    sa, sb, acc, top_, aos, ao, lts, lor,
    load, tok_send, tok_recv, q_send, q_recv, kv_send, kv_recv, y_send, m_send, halo_send, halo_recv,
    st_send, st_recv, cv_send, cv_recv, ao_send, ao_recv, lt_send, lt_recv,
):
    ways, group, tp, taps = sizes
    s = lax.axis_index("sp")
    t = lax.axis_index("tp")
    a = s // group
    g = s % group
    sp = ways * group
    other = 1 - t
    prow = nrm.shape[0]
    rows = PIECES * prow
    hd = qbuf.shape[2] // 2
    vdim = hgain_ref.shape[1]
    cch = conv.shape[2]
    channels = cch * tp
    half = hd // 2
    mate = a * group + g + 1 - 2 * (g % 2)
    across = a * group + (g + 2) % group
    stays = a % 2 == 0

    def turn(i):
        return g + (i % 2) * (group - 1 - 2 * g)

    def remote(src, dst, send, recv, row, col):
        return pltpu.make_async_remote_copy(
            src_ref=src, dst_ref=dst, send_sem=send, recv_sem=recv,
            device_id={"sp": row, "tp": col}, device_id_type=MESH)

    small = [
        pltpu.make_async_copy(src, dst, load.at[8 + n]) for n, (src, dst) in enumerate((
            (qkg_in, qkg_ref), (gain_in, gain_ref), (lam_in, lam_ref),
            (hgain_in, hgain_ref), (taps_in, taps_ref), (cgain_in, cgain_ref), (cshift_in, cshift_ref)))]
    tok_loads = [
        pltpu.make_async_copy(tokens_ref.at[pl.ds(j * prow, prow)], toks.at[j], load.at[j]) for j in range(2)]
    weight_loads = [
        pltpu.make_async_copy(ref, w.at[n], load.at[2 + n]) for n, ref in enumerate((wq_ref, wk_ref, wv_ref, wa_ref, wg_ref))]
    out_load = pltpu.make_async_copy(wo_ref, wo, load.at[7])
    for c in small[:2] + tok_loads[:1] + weight_loads[:3] + tok_loads[1:] + weight_loads[3:] + small[2:]:
        c.start()

    barrier = pltpu.get_barrier_semaphore()
    flat = s * tp + t

    def greet(n, carry):
        to = lax.rem(flat + n, sp * tp)
        pl.semaphore_signal(barrier, inc=1, device_id={"sp": to // tp, "tp": to % tp}, device_id_type=MESH)
        return carry

    lax.fori_loop(1, sp * tp, greet, 0)
    small[0].wait()
    which = lax.broadcasted_iota(jnp.int32, (half, prow), 0)
    inverse = jnp.zeros((half, prow), jnp.float32)
    for n in range(half):
        inverse = jnp.where(which == n, 10000.0 ** (-2.0 * n / hd), inverse)
    gains = [jnp.broadcast_to(qkg_ref[m:m + 1], (128, hd)).T for m in range(2)]

    def tables(pc, carry):
        place = s * rows + pc * prow + lax.broadcasted_iota(jnp.int32, (half, prow), 1)
        angles = place.astype(jnp.float32) * inverse
        cosine, sine = jnp.cos(angles), jnp.sin(angles)
        for m in range(2):
            tab[pc, m, 0] = gains[m][:half] * cosine
            tab[pc, m, 1] = gains[m][half:] * sine
            tab[pc, m, 2] = gains[m][half:] * cosine
            tab[pc, m, 3] = gains[m][:half] * sine
        return carry

    def tok_copy(j):
        return remote(
            tokens_ref.at[pl.ds(j * prow, prow)], toks.at[2 + j], tok_send.at[j], tok_recv.at[j], s, other)

    lax.fori_loop(0, PIECES, tables, 0)
    for n in range(ways):
        acc[n] = jnp.zeros_like(acc[n])
        top_[n] = jnp.full_like(top_[n], NEG)
    small[1].wait()

    def piece_of(n):
        return (t + (n // 2) * (1 - 2 * t)) * 2 + n % 2

    def kv_z(pc, d):
        h = lax.rem(a + d, ways)
        return remote(kvs.at[pc, h], kvbuf.at[s, pc], kv_send.at[pc, d - 1], kv_recv.at[s, pc], h * group + g, t)

    def q_z(pc, d):
        h = lax.rem(a + d, ways)
        return remote(qs.at[pc, h], qbuf.at[a, pc], q_send.at[pc, d], q_recv.at[a, pc], h * group + turn(a), t)

    def kv_wait(slot, pc):
        remote(kvs.at[pc, 0], kvbuf.at[slot, pc], kv_send.at[0, 0], kv_recv.at[slot, pc], s, other).wait_recv()

    def to_across(src, slot, pc, d):
        return remote(src, kvbuf.at[slot, pc], y_send.at[d, pc], kv_recv.at[slot, pc], across, t)

    def to_mate(src, slot, pc, d):
        return remote(src, kvbuf.at[slot, pc], m_send.at[d, pc], kv_recv.at[slot, pc], mate, t)

    def prepared(x, scale, pc):
        outs = []
        for m in range(2):
            f = x[m * hd:m * hd + half]
            b = x[m * hd + half:(m + 1) * hd]
            mean = (jnp.sum(f * f, axis=0, keepdims=True) + jnp.sum(b * b, axis=0, keepdims=True)) / hd
            r = lax.rsqrt(mean + 1e-06) * scale
            f = f * r
            b = b * r
            outs.append(f * tab[pc, m, 0] - b * tab[pc, m, 1])
            outs.append(b * tab[pc, m, 2] + f * tab[pc, m, 3])
        return jnp.concatenate(outs, axis=0)

    def relay_z(n):
        pc = piece_of(n)
        for d in range(1, ways):
            slot = lax.rem(a + ways - d, ways) * group + g
            kv_wait(slot, pc)
            to_across(kvbuf.at[slot, pc], slot, pc, d).start()
            to_mate(kvbuf.at[slot, pc], slot, pc, d).start()

    def relay_y(n):
        pc = piece_of(n)
        for d in range(ways):
            slot = lax.rem(a + ways - d, ways) * group + (g + 2) % group
            kv_wait(slot, pc)
            to_mate(kvbuf.at[slot, pc], slot, pc, ways + d).start()

    def product(k, n):
        for j in range(5):
            @pl.when(jnp.logical_and(n == 0, k == j))
            def _():
                weight_loads[j].wait()

        raw[k] = jnp.dot(nrm[...], w[k], preferred_element_type=jnp.float32)
        return n

    def project(n):
        pc = piece_of(n)
        x = toks[n].astype(jnp.float32)
        x = x * lax.rsqrt(jnp.mean(x * x, axis=-1, keepdims=True) + 1e-06) * gain_ref[...]
        nrm[...] = x.astype(jnp.bfloat16)
        lax.fori_loop(0, 3, product, n)

        def rounded(k, h):
            return raw[k, :, h * 2 * hd:(h + 1) * 2 * hd].astype(jnp.bfloat16).astype(jnp.float32)

        for h in range(ways):
            qs[pc, h] = prepared(rounded(0, h).T, hd ** -0.5, pc).astype(jnp.bfloat16)
            kvs[pc, h, :prow] = prepared(rounded(1, h).T, 1.0, pc).T.astype(jnp.bfloat16)
            kvs[pc, h, prow:] = rounded(2, h).T.astype(jnp.bfloat16)

    tok_loads[0].wait()
    project(0)
    pl.semaphore_wait(barrier, sp * tp - 1)
    for j in range(2):
        tok_copy(j).start()

    def front(n, carry):
        pc = piece_of(n)

        @pl.when(n == 1)
        def _():
            tok_loads[1].wait()

        @pl.when(n >= 2)
        def _():
            tok_copy(n - 2).wait_recv()

        @pl.when(n >= 1)
        def _():
            project(n)

        def send_queries():
            for d in range(1, ways):
                q_z(pc, d).start()

            @pl.when(jnp.logical_not(stays))
            def _():
                q_z(pc, 0).start()

        @pl.when(n >= 2)
        def _():
            send_queries()

        for d in range(1, ways):
            kv_z(pc, d).start()
        to_across(kvs.at[pc, a], s, pc, 0).start()
        to_mate(kvs.at[pc, a], s, pc, 0).start()

        @pl.when(n < 2)
        def _():
            send_queries()

        @pl.when(stays)
        def _():
            qbuf[a, pc] = qs[pc, a]

        kvbuf[s, pc] = kvs[pc, a]

        @pl.when(n == 1)
        def _():
            out_load.start()

        lax.fori_loop(3, 5, product, n)
        ga = raw[3].astype(jnp.bfloat16).astype(jnp.float32)
        gg = raw[4].astype(jnp.bfloat16).astype(jnp.float32)
        gated = (ga * jax.nn.sigmoid(gg)).astype(jnp.bfloat16)
        gext[pl.ds(pl.multiple_of(32 + pc * prow, 32), prow)] = gated.astype(jnp.float32)

        @pl.when(pc == PIECES - 1)
        def _():
            glast[...] = gated[prow - 32:]

        @pl.when(n >= 1)
        def _():
            relay_z(n - 1)

        @pl.when(n >= 2)
        def _():
            relay_y(n - 2)

        return carry

    halo_out = remote(glast, halo, halo_send.at[0], halo_recv.at[0], lax.rem(s + 1, sp), t)
    lax.fori_loop(0, PIECES, front, 0)

    for c in small[2:]:
        c.wait()

    @pl.when(s < sp - 1)
    def _():
        halo_out.start()

    def take_halo():
        @pl.when(s > 0)
        def _():
            halo_out.wait_recv()
            gext[0:32] = halo[...].astype(jnp.float32)

        @pl.when(s == 0)
        def _():
            gext[0:32] = jnp.zeros((32, cch), jnp.float32)

    def st_copy(r):
        return remote(st.at[r], str_.at[r], st_send.at[r], st_recv.at[r], s, other)

    def convolve(r, carry):
        plain = jnp.zeros((prow, 128), jnp.float32)
        square = jnp.zeros((prow, 128), jnp.float32)
        for c in range(cch // 128):
            lanes = slice(c * 128, (c + 1) * 128)
            window = gext[pl.ds(pl.multiple_of(r * prow, prow), prow + 32), lanes]
            total = jnp.zeros((prow, 128), jnp.float32)
            for k in range(8):
                turned = window if k == 0 else pltpu.roll(window, prow + 32 - k, 0)
                for j in range(taps):
                    place = 32 - (taps - 1) + j
                    if place % 8 == k:
                        total = total + taps_ref[j:j + 1, lanes] * turned[place - k:place - k + prow]
            conv[r, :, lanes] = total
            plain = plain + total
            square = square + total * total
        st[r, 0:1] = jnp.sum(plain.T, axis=0, keepdims=True)
        st[r, 1:2] = jnp.sum(square.T, axis=0, keepdims=True)
        st_copy(r).start()
        return carry

    lax.fori_loop(1, PIECES, convolve, 0)

    def cv_copy(j):
        return remote(cvo.at[other * 2 + j], cvr.at[j], cv_send.at[j], cv_recv.at[j], s, other)

    def normalize(r, carry):
        st_copy(r).wait_recv()
        both = st[r] + str_[r]
        mean = both[0:1] / channels
        scale = lax.rsqrt(both[1:2] / channels - mean * mean + 1e-05)
        mean = jnp.broadcast_to(mean, (128, prow)).T
        scale = jnp.broadcast_to(scale, (128, prow)).T
        for c in range(cch // 128):
            lanes = slice(c * 128, (c + 1) * 128)
            y = (conv[r, :, lanes] - mean) * scale * cgain_ref[:, lanes] + cshift_ref[:, lanes]
            cvo[r, :, lanes] = (y * jax.nn.sigmoid(y)).astype(jnp.bfloat16)
        return carry

    own = 2 * prow
    wide = wo.shape[1]
    step = wide // 4
    top = ways * tp * vdim

    def conv_part(n, carry):
        cols = pl.ds(pl.multiple_of(n * step, step), step)
        mine = wo[pl.ds(pl.multiple_of(top + t * cch, cch), cch), cols]
        theirs = wo[pl.ds(pl.multiple_of(top + other * cch, cch), cch), cols]
        macc[:, cols] = jnp.dot(
            cvo[pl.ds(t * 2, 2)].reshape(own, cch), mine, preferred_element_type=jnp.float32) + jnp.dot(
            cvr[...].reshape(own, cch), theirs, preferred_element_type=jnp.float32)
        return carry

    def mate_wait(n, carry):
        pc = piece_of(n)
        for b in range(ways):
            for e in range(2):
                slot = b * group + (mate - a * group + 2 * e) % group
                kv_wait(slot, pc)
        return carry

    def q_wait(i, pc):
        remote(qs.at[pc, 0], qbuf.at[i, pc], q_send.at[0, 0], q_recv.at[i, pc], s, other).wait_recv()

    def q_waits(i, carry):
        here = jnp.logical_and(i == a, stays)

        @pl.when(jnp.logical_not(here))
        def _():
            for pc in range(PIECES):
                q_wait(i, pc)

        return carry

    lax.fori_loop(0, 2, mate_wait, 0)
    lax.fori_loop(0, ways, q_waits, 0)

    lam = jnp.sum(
        jnp.where(lax.broadcasted_iota(jnp.int32, lam_ref.shape, 1) == a, lam_ref[...], 0.0), axis=1, keepdims=True)
    head = t * ways + a
    span = 2 * prow

    def ao_copy(i, hf, slot):
        return remote(aos.at[i, hf], ao.at[slot], ao_send.at[i, hf], ao_recv.at[slot], i * group + turn(i), hf)

    def lt_copy(i, slot):
        return remote(lts.at[i], lor.at[slot], lt_send.at[i], lt_recv.at[slot], i * group + turn(i), t)

    upper = a // (ways // 2)
    visits = []
    for k in range(ways - 1):
        n = k * upper + (ways - 2 - k) * (1 - upper)
        visits.append(jnp.where(n >= a, n + 1, n))
    visits.append(a)
    wide_edges = []
    edges = []
    for i in visits:
        wide_edges.append((wide_edges[-1] if wide_edges else 0) + (i * group + turn(i)) // 2)
        edges.append((edges[-1] if edges else 0) + i + 1)
    wide_items = balanced(ways, group) + ways
    steps = ways * (ways - 1) // 2 + ways
    wide_steps = wide_items // 2

    def item(x):
        x = jnp.minimum(x, wide_items + 2 * steps - 1)
        narrow = jnp.where(x >= wide_items, 1, 0)
        d = (x - wide_items) // 2
        last = narrow * (x % 2)
        q = jnp.where(narrow == 1, d, x - ways)
        k = 0
        base = 0
        for n in range(ways - 1):
            edge = jnp.where(narrow == 1, edges[n], wide_edges[n])
            k = jnp.where(q >= edge, n + 1, k)
            base = jnp.where(q >= edge, edge, base)
        k = jnp.where(q < 0, x, k)
        i = visits[-1]
        for n in range(ways - 1):
            i = jnp.where(k == n, visits[n], i)
        chunk = i * group + turn(i)
        j = jnp.where(narrow == 1, (q - base + i) % (i + 1), jnp.where(q < 0, chunk // 2, q - base))
        first = piece_of(2 * narrow + last)
        slots = [(j * (2 + 2 * narrow) + n // 2 + narrow * (n - n // 2), first + (1 - narrow) * (n % 2)) for n in range(4)]
        return i, chunk, slots

    def score(x, ref):
        i, _, slots = item(x)
        for m in range(2):
            queries = jnp.concatenate([qbuf[i, pc, m * hd:(m + 1) * hd, :] for pc in range(PIECES)], axis=1)
            keys = jnp.concatenate([kvbuf[p, q, :prow, m * hd:(m + 1) * hd] for p, q in slots], axis=0)
            ref[m] = jnp.dot(keys, queries, preferred_element_type=jnp.float32)

    def absorb(x, ref, masked):
        i, chunk, slots = item(x)
        vb = jnp.concatenate([kvbuf[p, q, prow:] for p, q in slots], axis=1)
        vb = jnp.concatenate([vb, jnp.ones((16, rows), jnp.bfloat16)], axis=0)
        for m in range(2):
            sc = ref[m]
            if masked:
                kp = lax.broadcasted_iota(jnp.int32, (prow, rows), 0)
                qp = lax.broadcasted_iota(jnp.int32, (prow, rows), 1)
                ahead = qp - kp
                sc = jnp.concatenate([
                    jnp.where(ahead >= (p - chunk) * rows + q * prow, sc[n * prow:(n + 1) * prow], NEG)
                    for n, (p, q) in enumerate(slots)], axis=0)
            old = top_[i, m:m + 1]
            new = jnp.maximum(old, jnp.max(sc, axis=0, keepdims=True))
            p = jnp.exp(sc - new)
            f = jnp.exp(old - new)
            acc[i, m] = acc[i, m] * f + jnp.dot(vb, p.astype(jnp.bfloat16), preferred_element_type=jnp.float32)
            top_[i, m:m + 1] = new

    def double(y, masked):
        score(2 * y + 1, sb)
        absorb(2 * y, sa, masked)
        score(2 * y + 2, sa)
        absorb(2 * y + 1, sb, masked)

    def attend(y, carry):
        d = y - wide_steps

        @pl.when(y == wide_steps - 1)
        def _():
            lax.fori_loop(2, 3, mate_wait, 0)

        @pl.when(y == wide_steps)
        def _():
            lax.fori_loop(3, 4, mate_wait, 0)

        masked = y < ways // 2
        for edge in edges[:-1]:
            masked = jnp.logical_or(masked, d == edge)
        masked = jnp.logical_or(masked, d == 0)

        @pl.when(masked)
        def _():
            double(y, True)

        @pl.when(jnp.logical_not(masked))
        def _():
            double(y, False)

        @pl.when(d >= 0)
        def _():
            for k in range(ways):
                @pl.when(d == edges[k] - 1)
                def _():
                    finish(visits[k])

        @pl.when(d < 0)
        def _():
            @pl.when(y == 1)
            def _():
                relay_z(3)

            @pl.when(y == 2)
            def _():
                take_halo()
                lax.fori_loop(0, 1, convolve, 0)

            @pl.when(y == 3)
            def _():
                relay_y(2)

            @pl.when(y == 6)
            def _():
                lax.fori_loop(0, PIECES, normalize, 0)
                for j in range(2):
                    cv_copy(j).start()

            @pl.when(y == 7)
            def _():
                relay_y(3)

        return carry

    def finish(i):
        l0 = acc[i, 0, vdim:vdim + 1]
        l1 = acc[i, 1, vdim:vdim + 1]
        heads = acc[i, 0, :vdim] / l0 - lam * acc[i, 1, :vdim] / l1
        heads = heads * lax.rsqrt(jnp.mean(heads * heads, axis=0, keepdims=True) + 1e-06)
        heads = (heads.T * hgain_ref[...]).astype(jnp.bfloat16)
        lts[i, 0:1] = top_[i, 0:1] + jnp.log(l0)
        lts[i, 1:2] = top_[i, 1:2] + jnp.log(l1)
        here = jnp.logical_and(i == a, stays)
        for hf in range(2):
            aos[i, hf] = heads[hf * own:(hf + 1) * own]
            mine = jnp.logical_and(here, t == hf)

            @pl.when(mine)
            def _():
                ao[head] = heads[hf * own:(hf + 1) * own]

            @pl.when(jnp.logical_not(mine))
            def _():
                ao_copy(i, hf, head).start()

        @pl.when(here)
        def _():
            lor[a] = lts[i]

        @pl.when(jnp.logical_not(here))
        def _():
            lt_copy(i, a).start()

    score(0, sa)
    lax.fori_loop(0, wide_steps + steps, attend, 0)
    out_load.wait()
    for j in range(2):
        cv_copy(j).wait_recv()
    lax.fori_loop(0, 4, conv_part, 0)

    def gather(h, carry):
        b = h % ways
        local = jnp.logical_and(jnp.logical_and(b == a, h // ways == t), stays)

        @pl.when(jnp.logical_not(local))
        def _():
            remote(aos.at[0, 0], ao.at[h], ao_send.at[0, 0], ao_recv.at[h], s, other).wait_recv()

        return carry

    lax.fori_loop(0, ways * tp, gather, 0)

    def att_part(n, carry):
        cols = pl.ds(pl.multiple_of(n * step, step), step)
        left = jnp.concatenate([ao[h] for h in range(ways * tp)], axis=1)
        mixed_ref[:, cols] = (
            macc[:, cols] + jnp.dot(left, wo[:top, cols], preferred_element_type=jnp.float32)).astype(jnp.bfloat16)
        return carry

    lax.fori_loop(0, 4, att_part, 0)

    for b in range(ways):
        local = jnp.logical_and(b == a, stays)

        @pl.when(jnp.logical_not(local))
        def _():
            remote(lts.at[0], lor.at[b], lt_send.at[0], lt_recv.at[b], s, other).wait_recv()

        for m in range(2):
            lo_ref[m, b:b + 1] = lor[b, m:m + 1]

    for j in range(2):
        tok_copy(j).wait_send()
        cv_copy(j).wait_send()

    def drain(pc, carry):
        for d in range(1, ways):
            kv_z(pc, d).wait_send()
            q_z(pc, d).wait_send()

        @pl.when(jnp.logical_not(stays))
        def _():
            q_z(pc, 0).wait_send()

        for d in range(ways):
            to_across(kvs.at[pc, 0], s, pc, d).wait_send()
        for d in range(2 * ways):
            to_mate(kvs.at[pc, 0], s, pc, d).wait_send()
        st_copy(pc).wait_send()
        return carry

    lax.fori_loop(0, PIECES, drain, 0)

    @pl.when(s < sp - 1)
    def _():
        halo_out.wait_send()

    def drain_out(i, carry):
        here = jnp.logical_and(i == a, stays)
        for hf in range(2):
            @pl.when(jnp.logical_not(jnp.logical_and(here, t == hf)))
            def _():
                ao_copy(i, hf, head).wait_send()

        @pl.when(jnp.logical_not(here))
        def _():
            lt_copy(i, a).wait_send()

        return carry

    lax.fori_loop(0, ways, drain_out, 0)


def whole_layer(
    sp, tp, tokens, norm_gain, query_weight, key_weight, value_weight, glu_value_weight, glu_gate_weight,
    qk_gain, mix_lambda, head_gain, conv_kernel, channel_gain, channel_shift, output_weight,
):
    ways = mix_lambda.shape[0]
    group = sp // ways
    own, width = tokens.shape
    rows = own * tp
    prow = rows // PIECES
    hd = qk_gain.shape[1]
    half = hd // 2
    vdim = head_gain.shape[0]
    taps, cch = conv_kernel.shape
    f32, bf16 = jnp.float32, jnp.bfloat16
    any_ = pl.BlockSpec(memory_space=pl.ANY)
    vm = pl.BlockSpec(memory_space=pltpu.VMEM)
    dma = pltpu.SemaphoreType.DMA
    return pl.pallas_call(
        lambda *refs: layer_kernel((ways, group, tp, taps), *refs),
        out_shape=(
            pltpu.VMEM((own, output_weight.shape[1]), bf16), pltpu.VMEM((2, ways, rows), f32)),
        in_specs=[any_] * 14,
        out_specs=(vm, vm),
        scratch_shapes=[
            pltpu.VMEM((1, width), f32),
            pltpu.VMEM(qk_gain.shape, f32),
            pltpu.VMEM((1, ways), f32),
            pltpu.VMEM((1, vdim), f32),
            pltpu.VMEM((taps, cch), f32),
            pltpu.VMEM((1, cch), f32),
            pltpu.VMEM((1, cch), f32),
            pltpu.VMEM((PIECES, prow, width), bf16),
            pltpu.VMEM((5,) + query_weight.shape, bf16),
            pltpu.VMEM((PIECES, 2, 4, half, prow), f32),
            pltpu.VMEM(output_weight.shape, bf16),
            pltpu.VMEM((prow, width), bf16),
            pltpu.VMEM((5, prow, cch), f32),
            pltpu.VMEM((PIECES, ways, 2 * hd, prow), bf16),
            pltpu.VMEM((PIECES, ways, prow + vdim, 2 * hd), bf16),
            pltpu.VMEM((ways, PIECES, 2 * hd, prow), bf16),
            pltpu.VMEM((sp, PIECES, prow + vdim, 2 * hd), bf16),
            pltpu.VMEM((32 + rows, cch), f32),
            pltpu.VMEM((32, cch), bf16),
            pltpu.VMEM((32, cch), bf16),
            pltpu.VMEM((PIECES, prow, cch), f32),
            pltpu.VMEM((PIECES, prow, cch), bf16),
            pltpu.VMEM((2, prow, cch), bf16),
            pltpu.VMEM((PIECES, 2, prow), f32),
            pltpu.VMEM((PIECES, 2, prow), f32),
            pltpu.VMEM((own, output_weight.shape[1]), f32),
            pltpu.VMEM((2, rows, rows), f32),
            pltpu.VMEM((2, rows, rows), f32),
            pltpu.VMEM((ways, 2, vdim + 16, rows), f32),
            pltpu.VMEM((ways, 2, rows), f32),
            pltpu.VMEM((ways, 2, own, vdim), bf16),
            pltpu.VMEM((ways * tp, own, vdim), bf16),
            pltpu.VMEM((ways, 2, rows), f32),
            pltpu.VMEM((ways, 2, rows), f32),
            dma((16,)), dma((2,)), dma((2,)),
            dma((PIECES, ways)), dma((ways, PIECES)), dma((PIECES, ways - 1)), dma((sp, PIECES)),
            dma((ways, PIECES)), dma((2 * ways, PIECES)), dma((1,)), dma((1,)),
            dma((PIECES,)), dma((PIECES,)), dma((2,)), dma((2,)),
            dma((ways, 2)), dma((ways * tp,)), dma((ways,)), dma((ways,)),
        ],
        compiler_params=pltpu.CompilerParams(
            collective_id=3, has_side_effects=True, vmem_limit_bytes=62000000),
        name="layer",
    )(
        tokens, norm_gain.reshape(1, width), query_weight, key_weight, value_weight, glu_value_weight, glu_gate_weight,
        qk_gain, mix_lambda.reshape(1, ways), head_gain.reshape(1, vdim), conv_kernel, channel_gain.reshape(1, cch),
        channel_shift.reshape(1, cch), output_weight)


def per_device(
    tokens, norm_gain, query_weight, key_weight, value_weight, glu_value_weight, glu_gate_weight,
    qk_gain, mix_lambda, head_gain, conv_kernel, channel_gain, channel_shift, output_weight,
):
    head_size = qk_gain.shape[1]
    heads_here = mix_lambda.shape[0]
    value_size = head_gain.shape[0]
    kernel_len = conv_kernel.shape[0]
    conv_here = conv_kernel.shape[1]
    width = tokens.shape[1]
    sp = lax.axis_size("sp")
    tp = lax.axis_size("tp")
    me = lax.axis_index("sp")
    t = lax.axis_index("tp")
    ways = heads_here
    group = sp // ways
    own = tokens.shape[0]
    rows = own * tp
    if tp == 2 and ways * group == sp and group == 4 and balanced(ways, group) % 2 == 0 and ways % 2 == 0 and ways == group and own == 256 and head_size == 64 and value_size == 128:
        return whole_layer(
            sp, tp, tokens, norm_gain, query_weight, key_weight, value_weight, glu_value_weight, glu_gate_weight,
            qk_gain, mix_lambda, head_gain, conv_kernel, channel_gain, channel_shift, output_weight)

    def norm(piece):
        inputs = piece.astype(jnp.float32)
        return (
            inputs * lax.rsqrt(jnp.mean(inputs * inputs, axis=-1, keepdims=True) + 1e-06) * norm_gain
        ).astype(jnp.bfloat16)

    others = [tokens] + [
        lax.ppermute(tokens, "tp", [(i, (i - d) % tp) for i in range(tp)]) for d in range(1, tp)
    ]
    if tp == 2:
        other = others[1]
        normed = norm(jnp.concatenate([jnp.where(t == 0, tokens, other), jnp.where(t == 0, other, tokens)], axis=0))
    else:
        stacked = jnp.stack(others)
        normed = norm(jnp.concatenate(
            [lax.dynamic_index_in_dim(stacked, (j - t) % tp, 0, keepdims=False) for j in range(tp)], axis=0))

    def turned(matrix):
        return lax.dot_general(matrix, normed, (((0,), (1,)), ((), ())), preferred_element_type=jnp.float32).astype(jnp.bfloat16)

    def plain(matrix):
        return jnp.dot(normed, matrix, preferred_element_type=jnp.float32).astype(jnp.bfloat16)

    positions = (me * rows + jnp.arange(rows, dtype=jnp.int32)).astype(jnp.float32)
    inverse = 10000.0 ** (-jnp.arange(0, head_size // 2, dtype=jnp.float32) * 2.0 / head_size)
    angles = positions[None, :] * inverse[:, None]
    cosine, sine = jnp.cos(angles)[None, None], jnp.sin(angles)[None, None]
    shape = (heads_here, 2, head_size, rows)
    rq = prepare_t(turned(query_weight).reshape(shape), qk_gain, cosine, sine) * jnp.bfloat16(head_size ** -0.5)
    rk = prepare_t(turned(key_weight).reshape(shape), qk_gain, cosine, sine)
    qt = rq.reshape(heads_here, 2 * head_size, rows)
    kk = jnp.transpose(rk.reshape(heads_here, 2 * head_size, rows), (0, 2, 1))
    vt = turned(value_weight).reshape(heads_here, value_size, rows)
    kv = jnp.concatenate([kk, vt.reshape(heads_here, value_size, rows // 128, 128).transpose(0, 2, 1, 3).reshape(heads_here, -1, 128)], axis=1)
    qall, kvall = spread(qt, kv, ways, group)

    glu_a, glu_g = plain(glu_value_weight), plain(glu_gate_weight)
    gated = (glu_a.astype(jnp.float32) * jax.nn.sigmoid(glu_g.astype(jnp.float32))).astype(jnp.bfloat16)
    earlier = from_behind(gated[rows - (kernel_len - 1):], "sp", 1)
    extended = jnp.concatenate([earlier, gated], axis=0).astype(jnp.float32)
    convolved = jnp.zeros((rows, conv_here), jnp.float32)
    for step in range(kernel_len):
        convolved = convolved + conv_kernel[step][None, :] * extended[step:step + rows]
    plain_sum, square_sum = lax.psum(
        (jnp.sum(convolved, axis=1), jnp.sum(convolved * convolved, axis=1)), "tp"
    )
    channels = conv_here * tp
    middle = (plain_sum / channels)[:, None]
    spread_ = (square_sum / channels)[:, None] - middle * middle
    conv_out = jax.nn.silu(
        (convolved - middle) * lax.rsqrt(spread_ + 1e-05) * channel_gain + channel_shift
    ).astype(jnp.bfloat16)

    place = (me % group).astype(jnp.int32).reshape(1)
    lam = lax.dynamic_slice(mix_lambda, (me // group,), (1,))
    att, lt = attention(place, lam, head_gain, qall, kvall)
    ao, lo, co = collect(
        att.reshape(ways, tp, own, value_size), lt, conv_out.reshape(tp, own, conv_here), ways, group, tp)
    heads = ways * tp
    merged = jnp.concatenate([
        jnp.transpose(ao, (1, 0, 2)).reshape(own, heads * value_size),
        jnp.transpose(co, (1, 0, 2)).reshape(own, channels)], axis=1)
    mixed = jnp.dot(merged, output_weight, preferred_element_type=jnp.float32).astype(jnp.bfloat16)
    return (mixed, jnp.transpose(lo, (1, 0, 2)))


def solution(mesh):
    placed = (
        P(("sp", "tp"), None), P(), P(None, "tp"), P(None, "tp"), P(None, "tp"), P(None, "tp"), P(None, "tp"),
        P(), P("tp"), P(), P(None, "tp"), P("tp"), P("tp"), P(),
    )
    return jax.shard_map(
        per_device,
        mesh=mesh,
        in_specs=placed,
        out_specs=(P(("sp", "tp"), None), P(None, "tp", "sp")),
        check_vma=False,
    )
```

```python
import math

import jax
import jax.numpy as jnp
from jax import lax
from jax.experimental import pallas as pl
from jax.experimental.pallas import tpu as pltpu
from jax.sharding import PartitionSpec as P

MESH = pl.DeviceIdType.MESH
NEG = -1e30


def from_behind(value, axis, steps):
    count = lax.axis_size(axis)
    leading, last = (max(0, -steps), min(count, count - steps))
    return lax.ppermute(value, axis, [(source, source + steps) for source in range(leading, last)])


def flipped(g, a, group):
    if group % 2:
        return g
    return jnp.where(a % 2 == 0, g, group - 1 - g)


def spread_kernel(ways, group, q_ref, kv_ref, qo_ref, kvo_ref, qsend, qrecv, ksend, kfwd, krelay, krecv, local):
    me = lax.axis_index("sp")
    a = me // group
    g = me % group
    cores = 2 if group % 2 == 0 else 1
    half = group // cores
    mate = a * group + (g + 1 - 2 * (g % 2)) if cores == 2 else me

    def same(d):
        return (g + d * cores) % group

    peers = [lax.rem(a + d, ways) * group + g for d in range(1, ways)]
    peers += [a * group + same(d) for d in range(1, half)]
    if cores == 2:
        peers.append(mate)
        peers += [lax.rem(a + d, ways) * group + group - 1 - g for d in range(ways)]
    barrier = pltpu.get_barrier_semaphore()
    for peer in peers:
        pl.semaphore_signal(barrier, inc=1, device_id={"sp": peer}, device_id_type=MESH)
    pl.semaphore_wait(barrier, len(peers))

    def kv_copy(src, slot, send, peer):
        return pltpu.make_async_remote_copy(
            src_ref=src, dst_ref=kvo_ref.at[slot], send_sem=send, recv_sem=krecv.at[slot],
            device_id={"sp": peer}, device_id_type=MESH)

    sends = []
    keep = pltpu.make_async_copy(kv_ref.at[a], kvo_ref.at[me], local.at[0])
    keep_q = pltpu.make_async_copy(q_ref.at[a], qo_ref.at[a], local.at[1])
    keep.start()

    def q_copy(h, slot, d):
        return pltpu.make_async_remote_copy(
            src_ref=q_ref.at[h], dst_ref=qo_ref.at[slot], send_sem=qsend.at[d], recv_sem=qrecv.at[slot],
            device_id={"sp": h * group + flipped(g, a, group)}, device_id_type=MESH)

    stays = a % 2 == 0 if cores == 2 else a >= 0

    @pl.when(stays)
    def _():
        keep_q.start()
    order = list(range(1, ways))
    for d in order:
        h = lax.rem(a + d, ways)
        c = kv_copy(kv_ref.at[h], me, ksend.at[d - 1], h * group + g)
        c.start()
        sends.append(c)

    def forward(d):
        src_a = lax.rem(a + ways - d, ways)
        slot = src_a * group + g
        if d:
            kv_copy(kvo_ref.at[slot], slot, ksend.at[d - 1], me).wait_recv()
            src = kvo_ref.at[slot]
        else:
            src = kv_ref.at[a]
        n = 0
        for e in range(1, half):
            c = kv_copy(src, slot, kfwd.at[d, n], a * group + same(e))
            c.start()
            sends.append(c)
            n += 1
        if cores == 2:
            c = kv_copy(src, slot, kfwd.at[d, n], mate)
            c.start()
            sends.append(c)

    def relay(d):
        src_a = lax.rem(a + ways - d, ways)
        for e in range(1, half):
            slot = src_a * group + same(e)
            kv_copy(kvo_ref.at[slot], slot, krelay.at[d, e - 1], mate).wait_recv()
            if cores == 2:
                c = kv_copy(kvo_ref.at[slot], slot, krelay.at[d, e - 1], mate)
                c.start()
                sends.append(c)

    forward(0)
    for d in order:
        c = q_copy(lax.rem(a + d, ways), a, d)
        c.start()
        sends.append(c)
    if cores == 2:
        @pl.when(jnp.logical_not(stays))
        def _():
            q_copy(a, a, 0).start()
    for d in range(1, ways):
        forward(d)
        relay(d - 1)
    relay(ways - 1)
    if cores == 2:
        for d in range(ways):
            src_a = lax.rem(a + ways - d, ways)
            for e in range(half):
                slot = src_a * group + (g + 1 - 2 * (g % 2) + e * cores) % group
                kv_copy(kvo_ref.at[slot], slot, krelay.at[0, 0], mate).wait_recv()
    for d in range(1, ways):
        src_a = lax.rem(a + ways - d, ways)
        q_copy(a, src_a, d).wait_recv()
    for c in sends:
        c.wait_send()
    keep.wait()

    @pl.when(stays)
    def _():
        keep_q.wait()

    if cores == 2:
        @pl.when(jnp.logical_not(stays))
        def _():
            q_copy(a, a, 0).wait()


def spread(q, kv, ways, group):
    cores = 2 if group % 2 == 0 else 1
    half = group // cores
    any_ = pl.BlockSpec(memory_space=pl.ANY)
    n = max(ways - 1, 1)
    return pl.pallas_call(
        lambda *refs: spread_kernel(ways, group, *refs),
        out_shape=(
            jax.ShapeDtypeStruct(q.shape, q.dtype),
            jax.ShapeDtypeStruct((ways * group,) + kv.shape[1:], kv.dtype),
        ),
        in_specs=[any_, any_],
        out_specs=(any_, any_),
        scratch_shapes=[
            pltpu.SemaphoreType.DMA((ways,)),
            pltpu.SemaphoreType.DMA((ways,)),
            pltpu.SemaphoreType.DMA((n,)),
            pltpu.SemaphoreType.DMA((ways, half)),
            pltpu.SemaphoreType.DMA((ways, max(half - 1, 1))),
            pltpu.SemaphoreType.DMA((ways * group,)),
            pltpu.SemaphoreType.DMA((2,)),
        ],
        compiler_params=pltpu.CompilerParams(collective_id=1, has_side_effects=True),
        name="spread",
    )(q, kv)


def collect_kernel(ways, group, tp, att_ref, lt_ref, conv_ref, ao_ref, lo_ref, co_ref, asend, arecv, lsend, lrecv, csend, crecv, local):
    me = lax.axis_index("sp")
    t = lax.axis_index("tp")
    a = me // group
    g = me % group
    vdim = att_ref.shape[-1]
    cch = conv_ref.shape[-1]

    def coords(i):
        dt, da = i % tp, i // tp
        return lax.rem(a + da, ways), lax.rem(t + dt, tp)

    total = ways * tp
    both = group % 2 == 0
    barrier = pltpu.get_barrier_semaphore()
    for i in range(total):
        pa, pt = coords(i)
        if i:
            pl.semaphore_signal(barrier, inc=1, device_id={"sp": pa * group + g, "tp": pt}, device_id_type=MESH)
        if both:
            pl.semaphore_signal(
                barrier, inc=1, device_id={"sp": pa * group + group - 1 - g, "tp": pt}, device_id_type=MESH)
    pl.semaphore_wait(barrier, 2 * total - 1 if both else total - 1)

    head = t * ways + a

    def att_copy(i, slot):
        pa, pt = coords(i)
        return pltpu.make_async_remote_copy(
            src_ref=att_ref.at[pa, pt], dst_ref=ao_ref.at[slot], send_sem=asend.at[i], recv_sem=arecv.at[slot],
            device_id={"sp": pa * group + flipped(g, pa, group), "tp": pt}, device_id_type=MESH)

    def lt_copy(i, slot):
        pa = lax.rem(a + i, ways)
        return pltpu.make_async_remote_copy(
            src_ref=lt_ref.at[pa], dst_ref=lo_ref.at[slot], send_sem=lsend.at[i], recv_sem=lrecv.at[slot],
            device_id={"sp": pa * group + flipped(g, pa, group), "tp": t}, device_id_type=MESH)

    stays = a % 2 == 0 if both else a >= 0
    sends = []
    for i in range(total - 1, 0, -1):
        c = att_copy(i, head)
        c.start()
        sends.append(c)
    for i in range(1, tp):
        pa, pt = coords(i)
        c = pltpu.make_async_remote_copy(
            src_ref=conv_ref.at[pt], dst_ref=co_ref.at[t],
            send_sem=csend.at[i], recv_sem=crecv.at[t],
            device_id={"sp": me, "tp": pt}, device_id_type=MESH)
        c.start()
        sends.append(c)
    for i in range(1, ways):
        c = lt_copy(i, a)
        c.start()
        sends.append(c)
    keep = pltpu.make_async_copy(conv_ref.at[t], co_ref.at[t], local.at[1])
    keep.start()
    mine = [
        pltpu.make_async_copy(att_ref.at[a, t], ao_ref.at[head], local.at[0]),
        pltpu.make_async_copy(lt_ref.at[a], lo_ref.at[a], local.at[2]),
    ]

    @pl.when(stays)
    def _():
        for c in mine:
            c.start()

    if both:
        @pl.when(jnp.logical_not(stays))
        def _():
            att_copy(0, head).start()
            lt_copy(0, a).start()
    for i in range(1, total):
        pa, pt = coords(i)
        att_copy(i, pt * ways + pa).wait_recv()
    for i in range(1, tp):
        pa, pt = coords(i)
        pltpu.make_async_remote_copy(
            src_ref=conv_ref.at[t], dst_ref=co_ref.at[pt],
            send_sem=csend.at[i], recv_sem=crecv.at[pt],
            device_id={"sp": me, "tp": pt}, device_id_type=MESH).wait_recv()
    for i in range(1, ways):
        lt_copy(i, lax.rem(a + i, ways)).wait_recv()
    for c in sends:
        c.wait_send()
    keep.wait()

    @pl.when(stays)
    def _():
        for c in mine:
            c.wait()

    if both:
        @pl.when(jnp.logical_not(stays))
        def _():
            att_copy(0, head).wait()
            lt_copy(0, a).wait()


def collect(att, lt, conv, ways, group, tp):
    any_ = pl.BlockSpec(memory_space=pl.ANY)
    rows, vdim = att.shape[2:]
    total = ways * tp
    return pl.pallas_call(
        lambda *refs: collect_kernel(ways, group, tp, *refs),
        out_shape=(
            jax.ShapeDtypeStruct((total, rows, vdim), att.dtype),
            jax.ShapeDtypeStruct(lt.shape, lt.dtype),
            jax.ShapeDtypeStruct(conv.shape, conv.dtype),
        ),
        in_specs=[any_] * 3,
        out_specs=(any_,) * 3,
        scratch_shapes=[
            pltpu.SemaphoreType.DMA((total,)),
            pltpu.SemaphoreType.DMA((total,)),
            pltpu.SemaphoreType.DMA((ways,)),
            pltpu.SemaphoreType.DMA((ways,)),
            pltpu.SemaphoreType.DMA((tp,)),
            pltpu.SemaphoreType.DMA((tp,)),
            pltpu.SemaphoreType.DMA((3,)),
        ],
        compiler_params=pltpu.CompilerParams(collective_id=2, has_side_effects=True),
        name="collect",
    )(att, lt, conv)


def attention(place, lam, head_gain, qt, kv, tile=512):
    ways, qdim, rows = qt.shape
    hd = qdim // 2
    blocks = kv.shape[0]
    vdim = head_gain.shape[0]
    group = blocks // ways
    tile = math.gcd(tile, rows)
    tiles = rows // tile
    def kernel(place_ref, lam_ref, gain_ref, q_ref, kv_ref, o_ref, lt_ref, sa, sb, acc_ref):
        i = pl.program_id(0); s = pl.program_id(1)
        chunk = i * group + flipped(place_ref[0], i, group)
        qs = [q_ref[0, m * hd:(m + 1) * hd, :] for m in range(2)]
        def score(j, ref):
            for m in range(2):
                ref[m] = jnp.dot(kv_ref[j, :rows, m * hd:(m + 1) * hd], qs[m], preferred_element_type=jnp.float32)
        def absorb(j, ref, tops, masked=False):
            vb = jnp.concatenate([kv_ref[j, rows + b * vdim:rows + (b + 1) * vdim] for b in range(rows // 128)], axis=1)
            vb = jnp.concatenate([vb, jnp.ones((16, rows), jnp.bfloat16)], axis=0)
            out=[]
            for m in range(2):
                sc = ref[m]
                if masked:
                    kp = lax.broadcasted_iota(jnp.int32, sc.shape, 0)
                    qp = lax.broadcasted_iota(jnp.int32, sc.shape, 1) + s * tile
                    sc = jnp.where(kp <= qp, sc, NEG)
                new = jnp.maximum(tops[m], jnp.max(sc, axis=0, keepdims=True))
                p = jnp.exp(sc - new)
                f = jnp.exp(tops[m] - new)
                acc_ref[m] = acc_ref[m] * f + jnp.dot(vb, p.astype(jnp.bfloat16), preferred_element_type=jnp.float32)
                out.append(new)
            return tuple(out)
        acc_ref[...] = jnp.zeros_like(acc_ref)
        one = jnp.full((1, tile), NEG, jnp.float32)
        score(chunk, sa)
        score(0, sb)
        tops = absorb(chunk, sa, (one, one), True)

        def pair(j, tops):
            score(2 * j + 1, sa)
            tops = absorb(2 * j, sb, tops)
            score(2 * j + 2, sb)
            return absorb(2 * j + 1, sa, tops)

        tops = lax.fori_loop(0, chunk // 2, pair, tops)
        tops = lax.cond(chunk % 2 == 1, lambda t: absorb(chunk - 1, sb, t), lambda t: t, tops)
        a0=acc_ref[0]; a1=acc_ref[1]
        t0,t1=tops
        l0=a0[vdim:vdim+1]; l1=a1[vdim:vdim+1]; a0=a0[:vdim]; a1=a1[:vdim]
        heads = a0 / l0 - lam_ref[0] * a1 / l1
        heads = heads * lax.rsqrt(jnp.mean(heads * heads, axis=0, keepdims=True) + 1e-06) * gain_ref[...]
        o_ref[0] = heads.T.astype(jnp.bfloat16)
        lt_ref[0, 0:1, :] = t0 + jnp.log(l0)
        lt_ref[0, 1:2, :] = t1 + jnp.log(l1)
    smem = pl.BlockSpec(memory_space=pltpu.SMEM)
    return pl.pallas_call(kernel, grid=(ways, tiles),
        out_shape=(jax.ShapeDtypeStruct((ways, rows, vdim), jnp.bfloat16), jax.ShapeDtypeStruct((ways, 2, rows), jnp.float32)),
        in_specs=[smem, smem, pl.BlockSpec((vdim, 1), lambda i, s: (0, 0)), pl.BlockSpec((1, qdim, tile), lambda i, s: (i, 0, s)), pl.BlockSpec(kv.shape, lambda i, s: (0, 0, 0))],
        out_specs=(pl.BlockSpec((1, tile, vdim), lambda i, s: (i, s, 0)), pl.BlockSpec((1, 2, tile), lambda i, s: (i, 0, s))),
        scratch_shapes=[pltpu.VMEM((2,rows,tile),jnp.float32),pltpu.VMEM((2,rows,tile),jnp.float32),pltpu.VMEM((2,vdim+16,tile),jnp.float32)],
        compiler_params=pltpu.CompilerParams(vmem_limit_bytes=58 << 20), name="attend")(place, lam, head_gain.reshape(-1, 1), qt, kv)


def prepare_t(raw, qk_gain, cosine, sine):
    values = raw.astype(jnp.float32)
    values = values * lax.rsqrt(jnp.mean(values * values, axis=2, keepdims=True) + 1e-06)
    values = values * qk_gain[None, :, :, None]
    half = raw.shape[2] // 2
    first, second = values[:, :, :half], values[:, :, half:]
    return jnp.concatenate(
        [first * cosine - second * sine, second * cosine + first * sine], axis=2
    ).astype(jnp.bfloat16)

PIECES = 4


def balanced(ways, group):
    counts = {
        sum((i * group + (g if i % 2 == 0 else group - 1 - g)) // 2 for i in range(ways)) for g in range(group)}
    return counts.pop() if len(counts) == 1 else 1


def layer_kernel(
    sizes, tokens_ref, gain_in, wq_ref, wk_ref, wv_ref, wa_ref, wg_ref, qkg_in, lam_in, hgain_in, taps_in,
    cgain_in, cshift_in, wo_ref, mixed_ref, lo_ref,
    gain_ref, qkg_ref, lam_ref, hgain_ref, taps_ref, cgain_ref, cshift_ref,
    toks, w, tab, wo, nrm, raw, qs, kvs, qbuf, kvbuf, gext, glast, halo, conv, cvo, cvr, st, str_, macc,
    sa, sb, acc, top_, aos, ao, lts, lor,
    load, tok_send, tok_recv, q_send, q_recv, kv_send, kv_recv, y_send, m_send, halo_send, halo_recv,
    st_send, st_recv, cv_send, cv_recv, ao_send, ao_recv, lt_send, lt_recv,
):
    ways, group, tp, taps = sizes
    s = lax.axis_index("sp")
    t = lax.axis_index("tp")
    a = s // group
    g = s % group
    sp = ways * group
    other = 1 - t
    prow = nrm.shape[0]
    rows = PIECES * prow
    hd = qbuf.shape[2] // 2
    vdim = hgain_ref.shape[1]
    cch = conv.shape[2]
    channels = cch * tp
    half = hd // 2
    mate = a * group + g + 1 - 2 * (g % 2)
    across = a * group + (g + 2) % group
    stays = a % 2 == 0

    def turn(i):
        return g + (i % 2) * (group - 1 - 2 * g)

    def remote(src, dst, send, recv, row, col):
        return pltpu.make_async_remote_copy(
            src_ref=src, dst_ref=dst, send_sem=send, recv_sem=recv,
            device_id={"sp": row, "tp": col}, device_id_type=MESH)

    small = [
        pltpu.make_async_copy(src, dst, load.at[8 + n]) for n, (src, dst) in enumerate((
            (qkg_in, qkg_ref), (gain_in, gain_ref), (lam_in, lam_ref),
            (hgain_in, hgain_ref), (taps_in, taps_ref), (cgain_in, cgain_ref), (cshift_in, cshift_ref)))]
    tok_loads = [
        pltpu.make_async_copy(tokens_ref.at[pl.ds(j * prow, prow)], toks.at[j], load.at[j]) for j in range(2)]
    weight_loads = [
        pltpu.make_async_copy(ref, w.at[n], load.at[2 + n]) for n, ref in enumerate((wq_ref, wk_ref, wv_ref, wa_ref, wg_ref))]
    out_load = pltpu.make_async_copy(wo_ref, wo, load.at[7])
    for c in small[:2] + tok_loads[:1] + weight_loads[:3] + tok_loads[1:] + weight_loads[3:] + small[2:]:
        c.start()

    barrier = pltpu.get_barrier_semaphore()
    flat = s * tp + t

    def greet(n, carry):
        to = lax.rem(flat + n, sp * tp)
        pl.semaphore_signal(barrier, inc=1, device_id={"sp": to // tp, "tp": to % tp}, device_id_type=MESH)
        return carry

    lax.fori_loop(1, sp * tp, greet, 0)
    small[0].wait()
    which = lax.broadcasted_iota(jnp.int32, (half, prow), 0)
    inverse = jnp.zeros((half, prow), jnp.float32)
    for n in range(half):
        inverse = jnp.where(which == n, 10000.0 ** (-2.0 * n / hd), inverse)
    gains = [jnp.broadcast_to(qkg_ref[m:m + 1], (128, hd)).T for m in range(2)]

    def tables(pc, carry):
        place = s * rows + pc * prow + lax.broadcasted_iota(jnp.int32, (half, prow), 1)
        angles = place.astype(jnp.float32) * inverse
        cosine, sine = jnp.cos(angles), jnp.sin(angles)
        for m in range(2):
            tab[pc, m, 0] = gains[m][:half] * cosine
            tab[pc, m, 1] = gains[m][half:] * sine
            tab[pc, m, 2] = gains[m][half:] * cosine
            tab[pc, m, 3] = gains[m][:half] * sine
        return carry

    def tok_copy(j):
        return remote(
            tokens_ref.at[pl.ds(j * prow, prow)], toks.at[2 + j], tok_send.at[j], tok_recv.at[j], s, other)

    lax.fori_loop(0, PIECES, tables, 0)
    for n in range(ways):
        acc[n] = jnp.zeros_like(acc[n])
        top_[n] = jnp.full_like(top_[n], NEG)
    small[1].wait()

    def piece_of(n):
        return (t + (n // 2) * (1 - 2 * t)) * 2 + n % 2

    def kv_z(pc, d):
        h = lax.rem(a + d, ways)
        return remote(kvs.at[pc, h], kvbuf.at[s, pc], kv_send.at[pc, d - 1], kv_recv.at[s, pc], h * group + g, t)

    def q_z(pc, d):
        h = lax.rem(a + d, ways)
        return remote(qs.at[pc, h], qbuf.at[a, pc], q_send.at[pc, d], q_recv.at[a, pc], h * group + turn(a), t)

    def kv_wait(slot, pc):
        remote(kvs.at[pc, 0], kvbuf.at[slot, pc], kv_send.at[0, 0], kv_recv.at[slot, pc], s, other).wait_recv()

    def to_across(src, slot, pc, d):
        return remote(src, kvbuf.at[slot, pc], y_send.at[d, pc], kv_recv.at[slot, pc], across, t)

    def to_mate(src, slot, pc, d):
        return remote(src, kvbuf.at[slot, pc], m_send.at[d, pc], kv_recv.at[slot, pc], mate, t)

    def prepared(x, scale, pc):
        outs = []
        for m in range(2):
            f = x[m * hd:m * hd + half]
            b = x[m * hd + half:(m + 1) * hd]
            mean = (jnp.sum(f * f, axis=0, keepdims=True) + jnp.sum(b * b, axis=0, keepdims=True)) / hd
            r = lax.rsqrt(mean + 1e-06) * scale
            f = f * r
            b = b * r
            outs.append(f * tab[pc, m, 0] - b * tab[pc, m, 1])
            outs.append(b * tab[pc, m, 2] + f * tab[pc, m, 3])
        return jnp.concatenate(outs, axis=0)

    def relay_z(n):
        pc = piece_of(n)
        for d in range(1, ways):
            slot = lax.rem(a + ways - d, ways) * group + g
            kv_wait(slot, pc)
            to_across(kvbuf.at[slot, pc], slot, pc, d).start()
            to_mate(kvbuf.at[slot, pc], slot, pc, d).start()

    def relay_y(n):
        pc = piece_of(n)
        for d in range(ways):
            slot = lax.rem(a + ways - d, ways) * group + (g + 2) % group
            kv_wait(slot, pc)
            to_mate(kvbuf.at[slot, pc], slot, pc, ways + d).start()

    def product(k, n):
        for j in range(5):
            @pl.when(jnp.logical_and(n == 0, k == j))
            def _():
                weight_loads[j].wait()

        raw[k] = jnp.dot(nrm[...], w[k], preferred_element_type=jnp.float32)
        return n

    def project(n):
        pc = piece_of(n)
        x = toks[n].astype(jnp.float32)
        x = x * lax.rsqrt(jnp.mean(x * x, axis=-1, keepdims=True) + 1e-06) * gain_ref[...]
        nrm[...] = x.astype(jnp.bfloat16)
        lax.fori_loop(0, 3, product, n)

        def rounded(k, h):
            return raw[k, :, h * 2 * hd:(h + 1) * 2 * hd].astype(jnp.bfloat16).astype(jnp.float32)

        for h in range(ways):
            qs[pc, h] = prepared(rounded(0, h).T, hd ** -0.5 / math.log(2.0), pc).astype(jnp.bfloat16)
            kvs[pc, h, :prow] = prepared(rounded(1, h).T, 1.0, pc).T.astype(jnp.bfloat16)
            kvs[pc, h, prow:] = rounded(2, h).T.astype(jnp.bfloat16)

    tok_loads[0].wait()
    project(0)
    pl.semaphore_wait(barrier, sp * tp - 1)
    for j in range(2):
        tok_copy(j).start()

    def front(n, carry):
        pc = piece_of(n)

        @pl.when(n == 1)
        def _():
            tok_loads[1].wait()

        @pl.when(n >= 2)
        def _():
            tok_copy(n - 2).wait_recv()

        @pl.when(n >= 1)
        def _():
            project(n)

        def send_queries():
            for d in range(1, ways):
                q_z(pc, d).start()

            @pl.when(jnp.logical_not(stays))
            def _():
                q_z(pc, 0).start()

        @pl.when(n >= 2)
        def _():
            send_queries()

        for d in range(1, ways):
            kv_z(pc, d).start()
        to_across(kvs.at[pc, a], s, pc, 0).start()
        to_mate(kvs.at[pc, a], s, pc, 0).start()

        @pl.when(n < 2)
        def _():
            send_queries()

        @pl.when(stays)
        def _():
            qbuf[a, pc] = qs[pc, a]

        kvbuf[s, pc] = kvs[pc, a]

        @pl.when(n == 1)
        def _():
            out_load.start()

        lax.fori_loop(3, 5, product, n)
        ga = raw[3].astype(jnp.bfloat16).astype(jnp.float32)
        gg = raw[4].astype(jnp.bfloat16).astype(jnp.float32)
        gated = (ga * jax.nn.sigmoid(gg)).astype(jnp.bfloat16)
        gext[pl.ds(pl.multiple_of(32 + pc * prow, 32), prow)] = gated.astype(jnp.float32)

        @pl.when(pc == PIECES - 1)
        def _():
            glast[...] = gated[prow - 32:]

        @pl.when(n >= 1)
        def _():
            relay_z(n - 1)

        @pl.when(n >= 2)
        def _():
            relay_y(n - 2)

        return carry

    halo_out = remote(glast, halo, halo_send.at[0], halo_recv.at[0], lax.rem(s + 1, sp), t)
    lax.fori_loop(0, PIECES, front, 0)

    for c in small[2:]:
        c.wait()

    @pl.when(s < sp - 1)
    def _():
        halo_out.start()

    def take_halo():
        @pl.when(s > 0)
        def _():
            halo_out.wait_recv()
            gext[0:32] = halo[...].astype(jnp.float32)

        @pl.when(s == 0)
        def _():
            gext[0:32] = jnp.zeros((32, cch), jnp.float32)

    def st_copy(r):
        return remote(st.at[r], str_.at[r], st_send.at[r], st_recv.at[r], s, other)

    def convolve(r, carry):
        plain = jnp.zeros((prow, 128), jnp.float32)
        square = jnp.zeros((prow, 128), jnp.float32)
        for c in range(cch // 128):
            lanes = slice(c * 128, (c + 1) * 128)
            window = gext[pl.ds(pl.multiple_of(r * prow, prow), prow + 32), lanes]
            total = jnp.zeros((prow, 128), jnp.float32)
            for k in range(8):
                turned = window if k == 0 else pltpu.roll(window, prow + 32 - k, 0)
                for j in range(taps):
                    place = 32 - (taps - 1) + j
                    if place % 8 == k:
                        total = total + taps_ref[j:j + 1, lanes] * turned[place - k:place - k + prow]
            conv[r, :, lanes] = total
            plain = plain + total
            square = square + total * total
        st[r, 0:1] = jnp.sum(plain.T, axis=0, keepdims=True)
        st[r, 1:2] = jnp.sum(square.T, axis=0, keepdims=True)
        st_copy(r).start()
        return carry

    lax.fori_loop(1, PIECES, convolve, 0)

    def cv_copy(j):
        return remote(cvo.at[other * 2 + j], cvr.at[j], cv_send.at[j], cv_recv.at[j], s, other)

    def normalize(r, carry):
        st_copy(r).wait_recv()
        both = st[r] + str_[r]
        mean = both[0:1] / channels
        scale = lax.rsqrt(both[1:2] / channels - mean * mean + 1e-05)
        mean = jnp.broadcast_to(mean, (128, prow)).T
        scale = jnp.broadcast_to(scale, (128, prow)).T
        for c in range(cch // 128):
            lanes = slice(c * 128, (c + 1) * 128)
            y = (conv[r, :, lanes] - mean) * scale * cgain_ref[:, lanes] + cshift_ref[:, lanes]
            cvo[r, :, lanes] = (y * jax.nn.sigmoid(y)).astype(jnp.bfloat16)
        return carry

    own = 2 * prow
    wide = wo.shape[1]
    step = wide // 4
    top = ways * tp * vdim

    def conv_part(n, carry):
        cols = pl.ds(pl.multiple_of(n * step, step), step)
        mine = wo[pl.ds(pl.multiple_of(top + t * cch, cch), cch), cols]
        theirs = wo[pl.ds(pl.multiple_of(top + other * cch, cch), cch), cols]
        macc[:, cols] = jnp.dot(
            cvo[pl.ds(t * 2, 2)].reshape(own, cch), mine, preferred_element_type=jnp.float32) + jnp.dot(
            cvr[...].reshape(own, cch), theirs, preferred_element_type=jnp.float32)
        return carry

    def mate_wait(n, carry):
        pc = piece_of(n)
        for b in range(ways):
            for e in range(2):
                slot = b * group + (mate - a * group + 2 * e) % group
                kv_wait(slot, pc)
        return carry

    def q_wait(i, pc):
        remote(qs.at[pc, 0], qbuf.at[i, pc], q_send.at[0, 0], q_recv.at[i, pc], s, other).wait_recv()

    def q_waits(i, carry):
        here = jnp.logical_and(i == a, stays)

        @pl.when(jnp.logical_not(here))
        def _():
            for pc in range(PIECES):
                q_wait(i, pc)

        return carry

    lax.fori_loop(0, 2, mate_wait, 0)
    lax.fori_loop(0, ways, q_waits, 0)

    lam = jnp.sum(
        jnp.where(lax.broadcasted_iota(jnp.int32, lam_ref.shape, 1) == a, lam_ref[...], 0.0), axis=1, keepdims=True)
    head = t * ways + a
    span = 2 * prow

    def ao_copy(i, hf, slot):
        return remote(aos.at[i, hf], ao.at[slot], ao_send.at[i, hf], ao_recv.at[slot], i * group + turn(i), hf)

    def lt_copy(i, slot):
        return remote(lts.at[i], lor.at[slot], lt_send.at[i], lt_recv.at[slot], i * group + turn(i), t)

    upper = a // (ways // 2)
    visits = []
    for k in range(ways - 1):
        n = k * upper + (ways - 2 - k) * (1 - upper)
        visits.append(jnp.where(n >= a, n + 1, n))
    visits.append(a)
    wide_edges = []
    edges = []
    for i in visits:
        wide_edges.append((wide_edges[-1] if wide_edges else 0) + (i * group + turn(i)) // 2)
        edges.append((edges[-1] if edges else 0) + i + 1)
    wide_items = balanced(ways, group) + ways
    steps = ways * (ways - 1) // 2 + ways
    wide_steps = wide_items // 2

    def item(x):
        x = jnp.minimum(x, wide_items + 2 * steps - 1)
        narrow = jnp.where(x >= wide_items, 1, 0)
        d = (x - wide_items) // 2
        last = narrow * (x % 2)
        q = jnp.where(narrow == 1, d, x - ways)
        k = 0
        base = 0
        for n in range(ways - 1):
            edge = jnp.where(narrow == 1, edges[n], wide_edges[n])
            k = jnp.where(q >= edge, n + 1, k)
            base = jnp.where(q >= edge, edge, base)
        k = jnp.where(q < 0, x, k)
        i = visits[-1]
        for n in range(ways - 1):
            i = jnp.where(k == n, visits[n], i)
        chunk = i * group + turn(i)
        j = jnp.where(narrow == 1, (q - base + i) % (i + 1), jnp.where(q < 0, chunk // 2, q - base))
        first = piece_of(2 * narrow + last)
        slots = [(j * (2 + 2 * narrow) + n // 2 + narrow * (n - n // 2), first + (1 - narrow) * (n % 2)) for n in range(4)]
        return i, chunk, slots

    def score(x, ref):
        i, _, slots = item(x)
        for m in range(2):
            queries = jnp.concatenate([qbuf[i, pc, m * hd:(m + 1) * hd, :] for pc in range(PIECES)], axis=1)
            keys = jnp.concatenate([kvbuf[p, q, :prow, m * hd:(m + 1) * hd] for p, q in slots], axis=0)
            ref[m] = jnp.dot(keys, queries, preferred_element_type=jnp.float32)

    def absorb(x, ref, masked):
        i, chunk, slots = item(x)
        vb = jnp.concatenate([kvbuf[p, q, prow:] for p, q in slots], axis=1)
        vb = jnp.concatenate([vb, jnp.ones((16, rows), jnp.bfloat16)], axis=0)
        for m in range(2):
            sc = ref[m]
            if masked:
                kp = lax.broadcasted_iota(jnp.int32, (prow, rows), 0)
                qp = lax.broadcasted_iota(jnp.int32, (prow, rows), 1)
                ahead = qp - kp
                sc = jnp.concatenate([
                    jnp.where(ahead >= (p - chunk) * rows + q * prow, sc[n * prow:(n + 1) * prow], NEG)
                    for n, (p, q) in enumerate(slots)], axis=0)
            old = top_[i, m:m + 1]
            new = jnp.maximum(old, jnp.max(sc, axis=0, keepdims=True))
            p = jnp.exp2(sc - new)
            f = jnp.exp2(old - new)
            acc[i, m] = acc[i, m] * f + jnp.dot(vb, p.astype(jnp.bfloat16), preferred_element_type=jnp.float32)
            top_[i, m:m + 1] = new

    def double(y, masked):
        score(2 * y + 1, sb)
        absorb(2 * y, sa, masked)
        score(2 * y + 2, sa)
        absorb(2 * y + 1, sb, masked)

    def masked_pair(y, carry):
        double(y, True)
        return carry

    def plain_pair(y, carry):
        double(y, False)
        return carry

    def attend(d, carry):
        masked = d == 0
        for edge in edges[:-1]:
            masked = jnp.logical_or(masked, d == edge)

        @pl.when(masked)
        def _():
            double(d + wide_steps, True)

        @pl.when(jnp.logical_not(masked))
        def _():
            double(d + wide_steps, False)

        done = d == edges[-1] - 1
        for edge in edges[:-1]:
            done = jnp.logical_or(done, d == edge - 1)

        @pl.when(done)
        def _():
            k = 0
            for n, edge in enumerate(edges[:-1]):
                k = jnp.where(d >= edge, n + 1, k)
            i = visits[-1]
            for n in range(ways - 1):
                i = jnp.where(k == n, visits[n], i)
            finish(i)

        return carry

    def finish(i):
        l0 = acc[i, 0, vdim:vdim + 1]
        l1 = acc[i, 1, vdim:vdim + 1]
        heads = acc[i, 0, :vdim] / l0 - lam * acc[i, 1, :vdim] / l1
        heads = heads * lax.rsqrt(jnp.mean(heads * heads, axis=0, keepdims=True) + 1e-06)
        heads = (heads.T * hgain_ref[...]).astype(jnp.bfloat16)
        lts[i, 0:1] = top_[i, 0:1] * math.log(2.0) + jnp.log(l0)
        lts[i, 1:2] = top_[i, 1:2] * math.log(2.0) + jnp.log(l1)
        here = jnp.logical_and(i == a, stays)
        for hf in range(2):
            aos[i, hf] = heads[hf * own:(hf + 1) * own]
            mine = jnp.logical_and(here, t == hf)

            @pl.when(mine)
            def _():
                ao[head] = heads[hf * own:(hf + 1) * own]

            @pl.when(jnp.logical_not(mine))
            def _():
                ao_copy(i, hf, head).start()

        @pl.when(here)
        def _():
            lor[a] = lts[i]

        @pl.when(jnp.logical_not(here))
        def _():
            lt_copy(i, a).start()

    score(0, sa)
    lax.fori_loop(0, ways // 2, masked_pair, 0)
    relay_z(3)
    cuts = (ways // 2, ways // 2 + 2, wide_steps - 2, wide_steps)
    lax.fori_loop(cuts[0], cuts[1], plain_pair, 0)
    take_halo()
    lax.fori_loop(0, 1, convolve, 0)
    relay_y(2)
    lax.fori_loop(cuts[1], cuts[2], plain_pair, 0)
    lax.fori_loop(0, PIECES, normalize, 0)
    for j in range(2):
        cv_copy(j).start()
    relay_y(3)
    lax.fori_loop(2, 3, mate_wait, 0)
    lax.fori_loop(cuts[2], cuts[3], plain_pair, 0)
    lax.fori_loop(3, 4, mate_wait, 0)
    lax.fori_loop(0, steps, attend, 0)
    out_load.wait()
    for j in range(2):
        cv_copy(j).wait_recv()
    lax.fori_loop(0, 4, conv_part, 0)

    def gather(n):
        b = lax.rem(a + n, ways)
        for e in range(tp):
            local = jnp.logical_and(stays, t == e) if n == 0 else False

            @pl.when(jnp.logical_not(local))
            def _():
                remote(
                    aos.at[0, 0], ao.at[e * ways + b], ao_send.at[0, 0], ao_recv.at[e * ways + b], s, other).wait_recv()

    def product_of(offsets, cols):
        heads = [e * ways + lax.rem(a + n, ways) for n in offsets for e in range(tp)]
        left = jnp.concatenate([ao[h] for h in heads], axis=1)
        right = jnp.concatenate([wo[pl.ds(pl.multiple_of(h * vdim, vdim), vdim), cols] for h in heads], axis=0)
        return jnp.dot(left, right, preferred_element_type=jnp.float32)

    for n in range(1, ways):
        gather(n)

    def far_part(n, carry):
        cols = pl.ds(pl.multiple_of(n * step, step), step)
        macc[:, cols] += product_of(range(1, ways), cols)
        return carry

    lax.fori_loop(0, 4, far_part, 0)
    gather(0)

    def att_part(n, carry):
        cols = pl.ds(pl.multiple_of(n * step, step), step)
        mixed_ref[:, cols] = (macc[:, cols] + product_of([0], cols)).astype(jnp.bfloat16)
        return carry

    lax.fori_loop(0, 4, att_part, 0)

    for b in range(ways):
        local = jnp.logical_and(b == a, stays)

        @pl.when(jnp.logical_not(local))
        def _():
            remote(lts.at[0], lor.at[b], lt_send.at[0], lt_recv.at[b], s, other).wait_recv()

        for m in range(2):
            lo_ref[m, b:b + 1] = lor[b, m:m + 1]

    for j in range(2):
        tok_copy(j).wait_send()
        cv_copy(j).wait_send()

    def drain(pc, carry):
        for d in range(1, ways):
            kv_z(pc, d).wait_send()
            q_z(pc, d).wait_send()

        @pl.when(jnp.logical_not(stays))
        def _():
            q_z(pc, 0).wait_send()

        for d in range(ways):
            to_across(kvs.at[pc, 0], s, pc, d).wait_send()
        for d in range(2 * ways):
            to_mate(kvs.at[pc, 0], s, pc, d).wait_send()
        st_copy(pc).wait_send()
        return carry

    lax.fori_loop(0, PIECES, drain, 0)

    @pl.when(s < sp - 1)
    def _():
        halo_out.wait_send()

    def drain_out(i, carry):
        here = jnp.logical_and(i == a, stays)
        for hf in range(2):
            @pl.when(jnp.logical_not(jnp.logical_and(here, t == hf)))
            def _():
                ao_copy(i, hf, head).wait_send()

        @pl.when(jnp.logical_not(here))
        def _():
            lt_copy(i, a).wait_send()

        return carry

    lax.fori_loop(0, ways, drain_out, 0)


def whole_layer(
    sp, tp, tokens, norm_gain, query_weight, key_weight, value_weight, glu_value_weight, glu_gate_weight,
    qk_gain, mix_lambda, head_gain, conv_kernel, channel_gain, channel_shift, output_weight,
):
    ways = mix_lambda.shape[0]
    group = sp // ways
    own, width = tokens.shape
    rows = own * tp
    prow = rows // PIECES
    hd = qk_gain.shape[1]
    half = hd // 2
    vdim = head_gain.shape[0]
    taps, cch = conv_kernel.shape
    f32, bf16 = jnp.float32, jnp.bfloat16
    any_ = pl.BlockSpec(memory_space=pl.ANY)
    vm = pl.BlockSpec(memory_space=pltpu.VMEM)
    dma = pltpu.SemaphoreType.DMA
    return pl.pallas_call(
        lambda *refs: layer_kernel((ways, group, tp, taps), *refs),
        out_shape=(
            pltpu.VMEM((own, output_weight.shape[1]), bf16), pltpu.VMEM((2, ways, rows), f32)),
        in_specs=[any_] * 14,
        out_specs=(vm, vm),
        scratch_shapes=[
            pltpu.VMEM((1, width), f32),
            pltpu.VMEM(qk_gain.shape, f32),
            pltpu.VMEM((1, ways), f32),
            pltpu.VMEM((1, vdim), f32),
            pltpu.VMEM((taps, cch), f32),
            pltpu.VMEM((1, cch), f32),
            pltpu.VMEM((1, cch), f32),
            pltpu.VMEM((PIECES, prow, width), bf16),
            pltpu.VMEM((5,) + query_weight.shape, bf16),
            pltpu.VMEM((PIECES, 2, 4, half, prow), f32),
            pltpu.VMEM(output_weight.shape, bf16),
            pltpu.VMEM((prow, width), bf16),
            pltpu.VMEM((5, prow, cch), f32),
            pltpu.VMEM((PIECES, ways, 2 * hd, prow), bf16),
            pltpu.VMEM((PIECES, ways, prow + vdim, 2 * hd), bf16),
            pltpu.VMEM((ways, PIECES, 2 * hd, prow), bf16),
            pltpu.VMEM((sp, PIECES, prow + vdim, 2 * hd), bf16),
            pltpu.VMEM((32 + rows, cch), f32),
            pltpu.VMEM((32, cch), bf16),
            pltpu.VMEM((32, cch), bf16),
            pltpu.VMEM((PIECES, prow, cch), f32),
            pltpu.VMEM((PIECES, prow, cch), bf16),
            pltpu.VMEM((2, prow, cch), bf16),
            pltpu.VMEM((PIECES, 2, prow), f32),
            pltpu.VMEM((PIECES, 2, prow), f32),
            pltpu.VMEM((own, output_weight.shape[1]), f32),
            pltpu.VMEM((2, rows, rows), f32),
            pltpu.VMEM((2, rows, rows), f32),
            pltpu.VMEM((ways, 2, vdim + 16, rows), f32),
            pltpu.VMEM((ways, 2, rows), f32),
            pltpu.VMEM((ways, 2, own, vdim), bf16),
            pltpu.VMEM((ways * tp, own, vdim), bf16),
            pltpu.VMEM((ways, 2, rows), f32),
            pltpu.VMEM((ways, 2, rows), f32),
            dma((16,)), dma((2,)), dma((2,)),
            dma((PIECES, ways)), dma((ways, PIECES)), dma((PIECES, ways - 1)), dma((sp, PIECES)),
            dma((ways, PIECES)), dma((2 * ways, PIECES)), dma((1,)), dma((1,)),
            dma((PIECES,)), dma((PIECES,)), dma((2,)), dma((2,)),
            dma((ways, 2)), dma((ways * tp,)), dma((ways,)), dma((ways,)),
        ],
        compiler_params=pltpu.CompilerParams(
            collective_id=3, has_side_effects=True, vmem_limit_bytes=62000000),
        name="layer",
    )(
        tokens, norm_gain.reshape(1, width), query_weight, key_weight, value_weight, glu_value_weight, glu_gate_weight,
        qk_gain, mix_lambda.reshape(1, ways), head_gain.reshape(1, vdim), conv_kernel, channel_gain.reshape(1, cch),
        channel_shift.reshape(1, cch), output_weight)


def per_device(
    tokens, norm_gain, query_weight, key_weight, value_weight, glu_value_weight, glu_gate_weight,
    qk_gain, mix_lambda, head_gain, conv_kernel, channel_gain, channel_shift, output_weight,
):
    head_size = qk_gain.shape[1]
    heads_here = mix_lambda.shape[0]
    value_size = head_gain.shape[0]
    kernel_len = conv_kernel.shape[0]
    conv_here = conv_kernel.shape[1]
    width = tokens.shape[1]
    sp = lax.axis_size("sp")
    tp = lax.axis_size("tp")
    me = lax.axis_index("sp")
    t = lax.axis_index("tp")
    ways = heads_here
    group = sp // ways
    own = tokens.shape[0]
    rows = own * tp
    if tp == 2 and ways * group == sp and group == 4 and balanced(ways, group) % 2 == 0 and ways % 2 == 0 and ways == group and own == 256 and head_size == 64 and value_size == 128:
        return whole_layer(
            sp, tp, tokens, norm_gain, query_weight, key_weight, value_weight, glu_value_weight, glu_gate_weight,
            qk_gain, mix_lambda, head_gain, conv_kernel, channel_gain, channel_shift, output_weight)

    def norm(piece):
        inputs = piece.astype(jnp.float32)
        return (
            inputs * lax.rsqrt(jnp.mean(inputs * inputs, axis=-1, keepdims=True) + 1e-06) * norm_gain
        ).astype(jnp.bfloat16)

    others = [tokens] + [
        lax.ppermute(tokens, "tp", [(i, (i - d) % tp) for i in range(tp)]) for d in range(1, tp)
    ]
    if tp == 2:
        other = others[1]
        normed = norm(jnp.concatenate([jnp.where(t == 0, tokens, other), jnp.where(t == 0, other, tokens)], axis=0))
    else:
        stacked = jnp.stack(others)
        normed = norm(jnp.concatenate(
            [lax.dynamic_index_in_dim(stacked, (j - t) % tp, 0, keepdims=False) for j in range(tp)], axis=0))

    def turned(matrix):
        return lax.dot_general(matrix, normed, (((0,), (1,)), ((), ())), preferred_element_type=jnp.float32).astype(jnp.bfloat16)

    def plain(matrix):
        return jnp.dot(normed, matrix, preferred_element_type=jnp.float32).astype(jnp.bfloat16)

    positions = (me * rows + jnp.arange(rows, dtype=jnp.int32)).astype(jnp.float32)
    inverse = 10000.0 ** (-jnp.arange(0, head_size // 2, dtype=jnp.float32) * 2.0 / head_size)
    angles = positions[None, :] * inverse[:, None]
    cosine, sine = jnp.cos(angles)[None, None], jnp.sin(angles)[None, None]
    shape = (heads_here, 2, head_size, rows)
    rq = prepare_t(turned(query_weight).reshape(shape), qk_gain, cosine, sine) * jnp.bfloat16(head_size ** -0.5)
    rk = prepare_t(turned(key_weight).reshape(shape), qk_gain, cosine, sine)
    qt = rq.reshape(heads_here, 2 * head_size, rows)
    kk = jnp.transpose(rk.reshape(heads_here, 2 * head_size, rows), (0, 2, 1))
    vt = turned(value_weight).reshape(heads_here, value_size, rows)
    kv = jnp.concatenate([kk, vt.reshape(heads_here, value_size, rows // 128, 128).transpose(0, 2, 1, 3).reshape(heads_here, -1, 128)], axis=1)
    qall, kvall = spread(qt, kv, ways, group)

    glu_a, glu_g = plain(glu_value_weight), plain(glu_gate_weight)
    gated = (glu_a.astype(jnp.float32) * jax.nn.sigmoid(glu_g.astype(jnp.float32))).astype(jnp.bfloat16)
    earlier = from_behind(gated[rows - (kernel_len - 1):], "sp", 1)
    extended = jnp.concatenate([earlier, gated], axis=0).astype(jnp.float32)
    convolved = jnp.zeros((rows, conv_here), jnp.float32)
    for step in range(kernel_len):
        convolved = convolved + conv_kernel[step][None, :] * extended[step:step + rows]
    plain_sum, square_sum = lax.psum(
        (jnp.sum(convolved, axis=1), jnp.sum(convolved * convolved, axis=1)), "tp"
    )
    channels = conv_here * tp
    middle = (plain_sum / channels)[:, None]
    spread_ = (square_sum / channels)[:, None] - middle * middle
    conv_out = jax.nn.silu(
        (convolved - middle) * lax.rsqrt(spread_ + 1e-05) * channel_gain + channel_shift
    ).astype(jnp.bfloat16)

    place = (me % group).astype(jnp.int32).reshape(1)
    lam = lax.dynamic_slice(mix_lambda, (me // group,), (1,))
    att, lt = attention(place, lam, head_gain, qall, kvall)
    ao, lo, co = collect(
        att.reshape(ways, tp, own, value_size), lt, conv_out.reshape(tp, own, conv_here), ways, group, tp)
    heads = ways * tp
    merged = jnp.concatenate([
        jnp.transpose(ao, (1, 0, 2)).reshape(own, heads * value_size),
        jnp.transpose(co, (1, 0, 2)).reshape(own, channels)], axis=1)
    mixed = jnp.dot(merged, output_weight, preferred_element_type=jnp.float32).astype(jnp.bfloat16)
    return (mixed, jnp.transpose(lo, (1, 0, 2)))


def solution(mesh):
    placed = (
        P(("sp", "tp"), None), P(), P(None, "tp"), P(None, "tp"), P(None, "tp"), P(None, "tp"), P(None, "tp"),
        P(), P("tp"), P(), P(None, "tp"), P("tp"), P("tp"), P(),
    )
    return jax.shard_map(
        per_device,
        mesh=mesh,
        in_specs=placed,
        out_specs=(P(("sp", "tp"), None), P(None, "tp", "sp")),
        check_vma=False,
    )
```
